256 devices in a mesh: grp: 2 (over y), kv: 16 (over z), tp: 8 (over x, core).
Axes of the slice: x: 4, y: 2, z: 16, core: 2. Of those that a mesh axis runs over, the one named last changes fastest.
The devices are a block of a 4x16x16 slice.
Arguments:
- tokens: bfloat16 [128, 4, 4096], P('grp', None, 'kv'), parts along dimension 0, may hold values from -13 to 13, as said below
- norm_gain: bfloat16 [4096], replicated, may hold values from 0.099609375 to 1.8984375
- w_query: bfloat16 [4096, 2048], P('kv', 'tp'), may hold values from -0.09375 to 0.09375
- w_key: bfloat16 [4096, 2048], P('kv', 'tp'), may hold values from -0.09375 to 0.09375
- w_value: bfloat16 [4096, 2048], P('kv', 'tp'), may hold values from -0.09375 to 0.09375
- w_outgate: bfloat16 [4096, 2048], P('kv', 'tp'), may hold values from -0.09375 to 0.09375
- gate_weight: bfloat16 [2, 4096, 16], replicated, may hold values from -0.09375 to 0.09375
- input_bias: float32 [16], P('tp'), may hold values from -1 to 1
- forget_bias: float32 [16], P('tp'), may hold values from -1 to 4
- w_out: bfloat16 [2048, 4096], P('tp', 'kv'), may hold values from -0.125 to 0.125
- saved_memory: float32 [128, 5, 16, 128, 128], P(('grp', 'kv'), None, 'tp'), parts along dimension 0, may hold values from -0.6 to 0.6
- saved_normalizer: float32 [128, 5, 16, 128], P(('grp', 'kv'), None, 'tp'), parts along dimension 0, may hold values from -0.6 to 0.6
- saved_stabilizer: float32 [128, 5, 16], P(('grp', 'kv'), None, 'tp'), parts along dimension 0, may hold values from -1 to 2
- accepted: int32 [128], P(('grp', 'kv')), parts along dimension 0, may hold values from 0 to 4
Outputs:
- mixed: bfloat16 [128, 4, 4096], P('grp', None, ('kv', 'tp')), parts along dimension 0
- new_memory: float32 [128, 5, 16, 128, 128], P(('grp', 'kv'), None, 'tp'), parts along dimension 0
- new_normalizer: float32 [128, 5, 16, 128], P(('grp', 'kv'), None, 'tp'), parts along dimension 0
- new_stabilizer: float32 [128, 5, 16], P(('grp', 'kv'), None, 'tp'), parts along dimension 0
The draws below stay inside these ranges and needn't reach their ends.
There are 2 independent parts, one for each index of `grp`. The reference program is written for one: setup_inputs(seed, part) draws one part's arguments, and reference() takes and returns one part's arrays. A program takes and returns all parts, laid end to end along the dimension named above; an argument that names none is the same for every part. Nothing has to cross between parts.
Inputs may be any that keep to these rules, and one draw needn't show every extreme that they name: `tokens`: the proposals' activations.
All inputs are finite; a program needn't handle non-finite values.
Results may differ from the reference program's by a relative error of at most 0.015.
The reference program's roundings to bfloat16 on the way (of `scaled` and `gated`) count: a program that leaves them out, or rounds other values in their place, can miss the bound.
Values may be sent and summed in bfloat16 or wider, within the bound.
No kernel may reach another device: no remote copies, remote signals or barrier semaphores. Data moves between devices by JAX's collectives and lax.ppermute only.
A program may use at most 64 MiB of HBM per device.

```python
import jax
import jax.numpy as jnp
from jax import lax

D = 4096
HEADS = 16
HEAD_DIM = 128
PROPOSALS = 4
SEQS = 64
SAVED = 5


def draw_tokens(key, part):
    ramp = jnp.exp(jnp.linspace(0.0, jnp.log(3.0), D))
    base = jnp.clip(jax.random.normal(key, (SEQS, PROPOSALS, D), jnp.float32), -4.0, 4.0)
    return (base * ramp).astype(jnp.bfloat16)


def plant(result, own_key, smallest, high):
    spot = [jax.random.randint(jax.random.fold_in(own_key, axis), (), 0, length) for axis, length in enumerate(result.shape)]
    widest = result.shape.index(max(result.shape))
    beside = spot[:widest] + [(spot[widest] + 1) % result.shape[widest]] + spot[widest + 1:]
    return result.at[tuple(spot)].set(smallest).at[tuple(beside)].set(high)


def level_of(stream_key, shape, cuts, smallest, high):
    def one(dim, blocks):
        steps = jax.random.uniform(jax.random.fold_in(jax.random.fold_in(stream_key, 6), dim), (blocks,), jnp.float32, smallest / len(cuts), high / len(cuts))
        return jnp.repeat(jnp.exp(steps), shape[dim] // blocks).reshape((-1,) + (1,) * (len(shape) - dim - 1))

    gain = one(*cuts[0])
    for cut in cuts[1:]:
        gain = gain * one(*cut)
    return gain


def noise(rng, shape, width, most, split=(), held_as=jnp.bfloat16):
    level = level_of(rng, shape, split, -0.22, 0.18) if split else 1.0
    array = jax.random.normal(rng, shape, jnp.float32) * width * level
    return jnp.minimum(jnp.maximum(array, -most), most).astype(held_as)


def setup_inputs(seed: int = 0, part: int = 0) -> dict:
    seeds = jax.random.split(jax.random.key(seed), 15)
    part_keys = jax.random.split(jax.random.fold_in(seeds[14], part), 15)
    tokens = draw_tokens(jax.random.fold_in(jax.random.fold_in(seeds[14], part), 71), part)
    norm_gain = jnp.clip(1.0 + 0.18 * jax.random.normal(seeds[1], (D,), jnp.float32), 0.099609375, 1.8984375).astype(jnp.bfloat16)
    w_query = noise(seeds[2], (D, HEADS * HEAD_DIM), D ** -0.5, 0.09375, ((0, 16), (1, 8)))
    w_key = noise(seeds[3], (D, HEADS * HEAD_DIM), D ** -0.5, 0.09375, ((0, 16), (1, 8)))
    w_value = noise(seeds[4], (D, HEADS * HEAD_DIM), D ** -0.5, 0.09375, ((0, 16), (1, 8)))
    w_outgate = noise(seeds[5], (D, HEADS * HEAD_DIM), D ** -0.5, 0.09375, ((0, 16), (1, 8)))
    gate_weight = noise(seeds[6], (2, D, HEADS), D ** -0.5, 0.09375)
    input_bias = jnp.clip(jax.random.uniform(seeds[7], (HEADS,), jnp.float32, -1.0, 1.0) * level_of(seeds[7], (HEADS,), ((0, 8),), -0.4, 0.0), -1.0, 1.0)
    forget_bias = jnp.clip(-1.0 + 5.0 * jax.random.uniform(seeds[8], (HEADS,), jnp.float32) ** level_of(seeds[8], (HEADS,), ((0, 8),), -0.2, 0.2), -1.0, 4.0)
    w_out = noise(seeds[9], (HEADS * HEAD_DIM, D), (HEADS * HEAD_DIM) ** -0.5, 0.125, ((0, 8), (1, 16)))
    saved_memory = noise(part_keys[10], (SEQS, SAVED, HEADS, HEAD_DIM, HEAD_DIM), 0.1, 0.6, ((0, 16), (2, 8)), jnp.float32)
    saved_normalizer = noise(part_keys[11], (SEQS, SAVED, HEADS, HEAD_DIM), 0.1, 0.6, ((0, 16), (2, 8)), jnp.float32)
    saved_stabilizer = jnp.clip(-1.0 + 3.0 * jax.random.uniform(part_keys[12], (SEQS, SAVED, HEADS), jnp.float32) ** level_of(part_keys[12], (SEQS, SAVED, HEADS), ((0, 16), (2, 8)), -0.2, 0.2), -1.0, 2.0)
    accepted = plant(jax.random.randint(part_keys[13], (SEQS,), 0, PROPOSALS + 1), jax.random.fold_in(part_keys[13], 1), 0, PROPOSALS).astype(jnp.int32)
    return {"tokens": tokens, "norm_gain": norm_gain, "w_query": w_query, "w_key": w_key, "w_value": w_value, "w_outgate": w_outgate, "gate_weight": gate_weight, "input_bias": input_bias, "forget_bias": forget_bias, "w_out": w_out, "saved_memory": saved_memory, "saved_normalizer": saved_normalizer, "saved_stabilizer": saved_stabilizer, "accepted": accepted}


EPSILON = 1e-06
HIGHEST = lax.Precision.HIGHEST

def advance(queries, key_rows, value_rows, in_gate, log_forget, memory, normalizer, stabilizer):
    key_scale = key_rows.shape[-1] ** (-0.5)
    outputs = []
    memories, normalizers, stabilizers = ([memory], [normalizer], [stabilizer])
    for position in range(queries.shape[1]):
        query_now = queries[:, position].astype(jnp.float32)
        key_now = key_rows[:, position].astype(jnp.float32) * key_scale
        value_now = value_rows[:, position].astype(jnp.float32)
        carried = log_forget[:, position] + stabilizer
        incoming = in_gate[:, position]
        top_value = jnp.maximum(carried, incoming)
        retain = jnp.exp(carried - top_value)
        admit_weight = jnp.exp(incoming - top_value)
        memory = retain[..., None, None] * memory + admit_weight[..., None, None] * (key_now[..., :, None] * value_now[..., None, :])
        normalizer = retain[..., None] * normalizer + admit_weight[..., None] * key_now
        stabilizer = top_value
        numerator = jnp.einsum('bhd,bhdv->bhv', query_now, memory, precision=HIGHEST)
        denominator = lax.optimization_barrier(jnp.sum(query_now * normalizer, -1))
        floor_value = jnp.exp(-stabilizer)
        outputs.append(numerator / jnp.maximum(jnp.abs(denominator), floor_value)[..., None])
        memories.append(memory)
        normalizers.append(normalizer)
        stabilizers.append(stabilizer)
    return (jnp.stack(outputs, 1), jnp.stack(memories, 1), jnp.stack(normalizers, 1), jnp.stack(stabilizers, 1))

def reference(tokens, norm_gain, w_query, w_key, w_value, w_outgate, gate_weight, input_bias, forget_bias, w_out, saved_memory, saved_normalizer, saved_stabilizer, accepted):
    seq_total, proposals, features = tokens.shape
    head_count = input_bias.shape[0]
    floats = tokens.astype(jnp.float32)
    inverse = lax.rsqrt(lax.optimization_barrier(jnp.mean(floats * floats, -1)) + EPSILON).reshape(-1, 1)
    scaled = (floats * norm_gain.astype(jnp.float32)).astype(jnp.bfloat16).reshape(-1, features)

    def project(weight):
        summed = jnp.dot(scaled, weight, preferred_element_type=jnp.float32) * inverse
        return summed.astype(jnp.bfloat16).reshape(seq_total, proposals, head_count, -1)
    queries = project(w_query)
    key_rows = project(w_key)
    value_rows = project(w_value)
    out_gate = project(w_outgate)
    gate_in = jnp.dot(scaled, gate_weight[0], preferred_element_type=jnp.float32) * inverse
    gate_forget = jnp.dot(scaled, gate_weight[1], preferred_element_type=jnp.float32) * inverse
    in_gate = gate_in.reshape(seq_total, proposals, head_count) + input_bias
    log_forget = jax.nn.log_sigmoid(gate_forget.reshape(seq_total, proposals, head_count) + forget_bias)
    chosen = accepted.astype(jnp.int32)
    memory = jnp.take_along_axis(saved_memory, chosen[:, None, None, None, None], 1)[:, 0]
    normalizer = jnp.take_along_axis(saved_normalizer, chosen[:, None, None, None], 1)[:, 0]
    stabilizer = jnp.take_along_axis(saved_stabilizer, chosen[:, None, None], 1)[:, 0]
    hidden, new_memory, new_normalizer, new_stabilizer = advance(queries, key_rows, value_rows, in_gate, log_forget, memory, normalizer, stabilizer)
    gated = (jax.nn.sigmoid(out_gate.astype(jnp.float32)) * hidden).astype(jnp.bfloat16)
    mixed = jnp.dot(gated.reshape(seq_total * proposals, -1), w_out, preferred_element_type=jnp.float32)
    mixed = mixed.astype(jnp.bfloat16).reshape(seq_total, proposals, features)
    return (mixed, new_memory, new_normalizer, new_stabilizer)
```

```python
import functools

import jax
import jax.numpy as jnp
from jax import lax
from jax.experimental import pallas as pl
from jax.experimental.pallas import tpu as pltpu
from jax.sharding import PartitionSpec as P

EPSILON = 1e-06
F32 = jnp.float32
BF16 = jnp.bfloat16


def iota(shape, dim):
    return lax.broadcasted_iota(jnp.int32, shape, dim)


def contract(a, b, da, db):
    return lax.dot_general(a, b, (((da,), (db,)), ((), ())), preferred_element_type=F32)


def project_kernel(place, tokens, gain, gates, wq, wk, wv, wo, out, *, owners):
    z, tp = place[0], place[1]
    seqs, props, width = tokens.shape
    rows = seqs * props
    per = rows // owners
    own = per // props
    x = tokens[...].astype(F32).reshape(rows, width)
    gain_rows = gain[...].astype(F32)
    pieces = []
    for j in range(width // 128):
        hit = iota(gain_rows.shape, 0) == z * (width // 128) + j
        pieces.append(jnp.sum(jnp.where(hit, gain_rows, 0.0), 0, keepdims=True))
    scaled = (x * jnp.concatenate(pieces, 1)).astype(BF16)
    r, c = iota((rows, rows), 0), iota((rows, rows), 1)
    source = (r // per) * per + (r % own) * props + (r % per) // own
    move = jnp.where(c == source, 1.0, 0.0).astype(BF16)
    scaled = contract(move, scaled, 1, 0).astype(BF16)
    block = 0
    for w in (wq, wk, wv, wo):
        y = contract(scaled, w[...], 1, 0).astype(BF16)
        for h in range(y.shape[1] // 128):
            out[:, block * per : (block + 1) * per, :] = y[:, h * 128 : (h + 1) * 128].reshape(owners, per, 128)
            block += 1
    heads = gates.shape[1]
    local = 2
    pick_r, pick_c = iota((8, 2 * heads), 0), iota((8, 2 * heads), 1)
    want = ((pick_r % 4) // local) * heads + tp * local + pick_r % local
    pick = jnp.where(pick_c == want, 1.0, 0.0).astype(BF16)
    own_gates = contract(pick, gates[...].reshape(2 * heads, width), 1, 0).astype(BF16)
    g = contract(own_gates, scaled, 1, 1)
    square = x * x
    s_hi = square.astype(BF16)
    s_lo = (square - s_hi.astype(F32)).astype(BF16)
    ones = jnp.ones((8, width), BF16)
    s = contract(ones, contract(move, s_hi, 1, 0).astype(BF16), 1, 1)
    s += contract(ones, contract(move, s_lo, 1, 0).astype(BF16), 1, 1)

    def words(value, split):
        hi = value.astype(BF16).astype(F32)
        return jnp.where(iota(value.shape, 0) < split, hi, value - hi)

    g, s = words(g, 4), words(s, 1)
    lanes = iota((8, 128), 1)
    span = 128 // per
    for half in range(rows // 128):
        gh = g[:, half * 128 : (half + 1) * 128]
        sh = pltpu.roll(s[:, half * 128 : (half + 1) * 128], 64, 1)
        low = jnp.where(lanes < 64, gh, sh).astype(BF16)
        high = jnp.where(lanes < 64, sh, gh).astype(BF16)
        for k in range(span):
            out[half * span + k, block * per :, :] = low if k < span // 2 else high


def cell_kernel(place, accepted, stab, ib, fb, got, m0, n0, gated, kv_out, coef, new_n, new_s, *, features):
    z = place[0]
    owners = got.shape[0]
    own, _, heads, dim, _ = m0.shape
    total = got[0].astype(F32)
    for k in range(1, owners):
        total = total + got[k].astype(F32)
    per = (total.shape[0] - 8) // (4 * heads)
    props = per // own
    small = total[4 * heads * per :]
    shift = (z % (128 // per)) * per
    small = pltpu.roll(small, lax.rem(128 - shift, 128), 1)
    g = small + pltpu.roll(small, 4, 0)
    sq = pltpu.roll(small + pltpu.roll(small, 7, 0), 64, 1)
    packed = jnp.where(iota(g.shape, 0) < 4, g, pltpu.roll(sq, 4, 0))
    cols = packed.T[:per]
    inverse = lax.rsqrt(cols[:, 4:5] / features + EPSILON)
    col = iota((per, heads), 1)
    ibv = jnp.where(col == 0, ib[0], ib[1])
    fbv = jnp.where(col == 0, fb[0], fb[1])
    in_gate = cols[:, 0:2] * inverse + ibv
    f = cols[:, 2:4] * inverse + fbv
    log_forget = jnp.minimum(f, 0.0) - jnp.log1p(jnp.exp(-jnp.abs(f)))
    srow, scol = iota((own, heads), 0), iota((own, heads), 1)
    m = jnp.zeros((own, heads), F32)
    for b in range(own):
        for h in range(heads):
            m = jnp.where((srow == b) & (scol == h), stab[b, h, accepted[b]], m)
    stabs, retain, admit = [m], [], []
    for t in range(props):
        carried = log_forget[t * own : (t + 1) * own] + m
        incoming = in_gate[t * own : (t + 1) * own]
        top = jnp.maximum(carried, incoming)
        retain.append(jnp.exp(carried - top))
        admit.append(jnp.exp(incoming - top))
        m = top
        stabs.append(m)
    scale = dim ** (-0.5)
    rr = iota((per, dim), 0) % own
    outs = []
    for h in range(heads):

        def part(kind):
            at = (kind * heads + h) * per
            return (total[at : at + per] * inverse).astype(BF16)

        q, k, v, o = part(0), part(1), part(2), part(3)
        kv_out[h] = k
        kv_out[heads + h] = v
        qf, kf, vf = q.astype(F32), k.astype(F32) * scale, v.astype(F32)
        base = jnp.zeros((per, dim), F32)
        for b in range(own):
            mine = jnp.where(rr == b, qf, 0.0).astype(BF16)
            mem = m0[b, 0, h]
            hi = mem.astype(BF16)
            lo = (mem - hi.astype(F32)).astype(BF16)
            base += contract(mine, hi, 1, 0) + contract(mine, lo, 1, 0)
        norm = n0[:, h, :]
        new_n[:, 0, h, :] = norm
        rows = []
        for t in range(props):
            sl = slice(t * own, (t + 1) * own)
            rt, at = retain[t][:, h : h + 1], admit[t][:, h : h + 1]
            norm = rt * norm + at * kf[sl]
            new_n[:, t + 1, h, :] = norm
            den = jnp.sum(qf[sl] * norm, -1, keepdims=True)
            weight = jnp.ones((own, 1), F32)
            num = jnp.zeros((own, dim), F32)
            for s in range(t, -1, -1):
                ss = slice(s * own, (s + 1) * own)
                dots = jnp.sum(qf[sl] * kf[ss], -1, keepdims=True)
                num += (weight * admit[s][:, h : h + 1] * dots) * vf[ss]
                weight = weight * retain[s][:, h : h + 1]
            num += weight * base[sl]
            floor = jnp.exp(-stabs[t + 1][:, h : h + 1])
            rows.append(num / jnp.maximum(jnp.abs(den), floor))
        hidden = jnp.concatenate(rows, 0)
        outs.append(jax.nn.sigmoid(o.astype(F32)) * hidden)
    gated[...] = jnp.concatenate(outs, 1).astype(BF16)
    for t in range(props):
        coef[t] = jnp.concatenate([retain[t], admit[t]], 1)
    for t in range(props + 1):
        new_s[t] = stabs[t]


def memory_kernel(accepted, coef, m0, kv, out, *, heads):
    b = pl.program_id(0)
    _, steps, _, dim, _ = out.shape
    per = kv.shape[1]
    props = steps - 1
    own = per // props
    scale = dim ** (-0.5)
    for h in range(heads):
        key = kv[h].astype(F32) * scale
        value = kv[heads + h].astype(F32)
        memory = m0[0, 0, h]
        out[0, 0, h] = memory
        row = iota((per, dim), 0)
        keys = key.T
        for t in range(props):
            hit = row == t * own + b
            vrow = jnp.sum(jnp.where(hit, value, 0.0), 0, keepdims=True)
            lane = iota(keys.shape, 1)
            kcol = jnp.sum(jnp.where(lane == t * own + b, keys, 0.0), 1, keepdims=True)
            memory = coef[t, b, h] * memory + (coef[t, b, heads + h] * kcol) * vrow
            out[0, t + 1, h] = memory


def mix_kernel(gathered, w, out, *, owners, props):
    rows = gathered.shape[0]
    per = rows // owners
    own = per // props
    y = contract(w[...], gathered[...], 0, 1).astype(BF16)
    r, c = iota((rows, rows), 0), iota((rows, rows), 1)
    t, rest = c // (rows // props), c % (rows // props)
    source = (rest // own) * per + t * own + rest % own
    move = jnp.where(r == source, 1.0, 0.0).astype(BF16)
    y = contract(y, move, 1, 0).astype(BF16)
    out[...] = y.reshape(out.shape)


def finish_kernel(got, out):
    total = got[0].astype(F32)
    for k in range(1, got.shape[0]):
        total = total + got[k].astype(F32)
    props, _, seqs = out.shape
    for t in range(props):
        out[t] = total[:, t * seqs : (t + 1) * seqs].astype(BF16)


SMEM = pl.BlockSpec(memory_space=pltpu.SMEM)


def local(
    tokens,
    norm_gain,
    w_query,
    w_key,
    w_value,
    w_outgate,
    gate_weight,
    input_bias,
    forget_bias,
    w_out,
    saved_memory,
    saved_normalizer,
    saved_stabilizer,
    accepted,
):
    owners, peers = lax.axis_size("kv"), lax.axis_size("tp")
    seqs, props, width = tokens.shape
    heads = input_bias.shape[0]
    own, saved, _, dim, _ = saved_memory.shape
    columns = w_query.shape[1]
    per = own * props
    z = lax.axis_index("kv")
    place = jnp.stack([z, lax.axis_index("tp")]).astype(jnp.int32)
    blocks = 4 * columns // 128

    gates = gate_weight.transpose(0, 2, 1)
    all_heads = gates.shape[1]

    def whole(shape):
        return pl.BlockSpec(shape, lambda *_: (0,) * len(shape))

    send = pl.pallas_call(
        functools.partial(project_kernel, owners=owners),
        grid_spec=pltpu.PrefetchScalarGridSpec(
            num_scalar_prefetch=1,
            grid=(1,),
            in_specs=[
                whole(tokens.shape),
                whole((norm_gain.shape[0] // 128, 128)),
                pl.BlockSpec((2, all_heads, width), lambda i, p: (0, 0, p[0])),
            ]
            + [whole(w_query.shape)] * 4,
            out_specs=whole((owners, blocks * per + 8, 128)),
        ),
        out_shape=jax.ShapeDtypeStruct((owners, blocks * per + 8, 128), BF16),
        name="project",
    )(place, tokens, norm_gain.reshape(-1, 128), gates, w_query, w_key, w_value, w_outgate)

    got = lax.all_to_all(send, "kv", split_axis=0, concat_axis=0, tiled=True)

    rows_n = jnp.take_along_axis(saved_normalizer, accepted[:, None, None, None], 1)[:, 0]
    m0 = jnp.take_along_axis(saved_memory, accepted[:, None, None, None, None], 1)
    stab = saved_stabilizer.transpose(0, 2, 1)
    gated, kv, coef, new_n, new_s = pl.pallas_call(
        functools.partial(cell_kernel, features=float(owners * width)),
        in_specs=[SMEM] * 5 + [pl.BlockSpec(memory_space=pltpu.VMEM)] * 3,
        out_specs=[pl.BlockSpec(memory_space=pltpu.VMEM)] * 5,
        out_shape=[
            jax.ShapeDtypeStruct((per, columns), BF16),
            jax.ShapeDtypeStruct((2 * heads, per, dim), BF16),
            jax.ShapeDtypeStruct((props, own, 2 * heads), F32),
            jax.ShapeDtypeStruct((own, props + 1, heads, dim), F32),
            jax.ShapeDtypeStruct((props + 1, own, heads), F32),
        ],
        name="cell",
    )(place, accepted, stab, input_bias, forget_bias, got, m0, rows_n)

    gathered = lax.all_gather(gated, "kv", axis=0, tiled=True)

    terms = pl.pallas_call(
        functools.partial(mix_kernel, owners=owners, props=props),
        in_specs=[pl.BlockSpec(memory_space=pltpu.VMEM)] * 2,
        out_specs=pl.BlockSpec(memory_space=pltpu.VMEM),
        out_shape=jax.ShapeDtypeStruct((peers, w_out.shape[1] // peers, seqs * props), BF16),
        name="mix",
    )(gathered, w_out)
    arrived = lax.all_to_all(terms, "tp", split_axis=0, concat_axis=0, tiled=True)

    new_memory = pl.pallas_call(
        functools.partial(memory_kernel, heads=heads),
        grid_spec=pltpu.PrefetchScalarGridSpec(
            num_scalar_prefetch=1,
            grid=(own,),
            in_specs=[
                SMEM,
                pl.BlockSpec((1, 1, heads, dim, dim), lambda b, a: (b, a[b], 0, 0, 0)),
                whole((2 * heads, per, dim)),
            ],
            out_specs=pl.BlockSpec((1, props + 1, heads, dim, dim), lambda b, a: (b, 0, 0, 0, 0)),
        ),
        out_shape=jax.ShapeDtypeStruct((own, props + 1, heads, dim, dim), F32),
        cost_estimate=pl.CostEstimate(flops=10_000_000, bytes_accessed=3_200_000, transcendentals=0),
        name="memory",
    )(accepted, coef, saved_memory, kv)

    mixed = pl.pallas_call(
        finish_kernel,
        in_specs=[pl.BlockSpec(memory_space=pltpu.VMEM)],
        out_specs=pl.BlockSpec(memory_space=pltpu.VMEM),
        out_shape=jax.ShapeDtypeStruct((props, w_out.shape[1] // peers, seqs), BF16),
        name="finish",
    )(arrived)
    return mixed.transpose(2, 0, 1), new_memory, new_n, new_s.transpose(1, 0, 2)


def solution(mesh):
    return jax.shard_map(
        local,
        mesh=mesh,
        in_specs=(
            P("grp", None, "kv"),
            P(),
            P("kv", "tp"),
            P("kv", "tp"),
            P("kv", "tp"),
            P("kv", "tp"),
            P(),
            P("tp"),
            P("tp"),
            P("tp", "kv"),
            P(("grp", "kv"), None, "tp", None, None),
            P(("grp", "kv"), None, "tp", None),
            P(("grp", "kv"), None, "tp"),
            P(("grp", "kv")),
        ),
        out_specs=(
            P("grp", None, ("kv", "tp")),
            P(("grp", "kv"), None, "tp", None, None),
            P(("grp", "kv"), None, "tp", None),
            P(("grp", "kv"), None, "tp"),
        ),
        check_vma=False,
    )
```

```python
import functools

import jax
import jax.numpy as jnp
from jax import lax
from jax.experimental import pallas as pl
from jax.experimental.pallas import tpu as pltpu
from jax.sharding import PartitionSpec as P

EPSILON = 1e-06
F32 = jnp.float32
BF16 = jnp.bfloat16
SHIFT = 2.0**20


def iota(shape, dim):
    return lax.broadcasted_iota(jnp.int32, shape, dim)


def contract(a, b, da, db):
    return lax.dot_general(a, b, (((da,), (db,)), ((), ())), preferred_element_type=F32)


def coded(x):
    y = x * SHIFT
    return ((y * jnp.abs(y)) * (y * y)).astype(BF16)


def decoded(y):
    y = y.astype(F32)
    root = lax.rsqrt(lax.rsqrt(jnp.maximum(jnp.abs(y), 1e-37)))
    return jnp.where(y < 0.0, -root, root)


def project_kernel(tokens, gain, wq, wk, wv, wo, gates_hbm, out, gates, sem, *, owners):
    z, tp = lax.axis_index("kv"), lax.axis_index("tp")
    seqs, props, width = tokens.shape
    fetch = pltpu.make_async_copy(gates_hbm.at[:, :, pl.ds(pl.multiple_of(z * width, width), width)], gates, sem)
    fetch.start()
    rows = seqs * props
    per = rows // owners
    own = per // props
    x = tokens[...].astype(F32).reshape(rows, width)
    gain_rows = gain[...].astype(F32)
    pieces = []
    for j in range(width // 128):
        hit = iota(gain_rows.shape, 0) == z * (width // 128) + j
        pieces.append(jnp.sum(jnp.where(hit, gain_rows, 0.0), 0, keepdims=True))
    scaled = (x * jnp.concatenate(pieces, 1)).astype(BF16)
    r, c = iota((rows, rows), 0), iota((rows, rows), 1)
    source = (r & -per) + (r & (own - 1)) * props + ((r & (per - 1)) >> log2(own))
    move = jnp.where(c == source, 1.0, 0.0).astype(BF16)
    scaled = contract(move, scaled, 1, 0).astype(BF16)
    block = 0
    for w in (wq, wk, wv, wo):
        y = coded(contract(scaled, w[...], 1, 0))
        for h in range(y.shape[1] // 128):
            out[:, block * per : (block + 1) * per, :] = y[:, h * 128 : (h + 1) * 128].reshape(owners, per, 128)
            block += 1
    square = x * x
    s_hi = square.astype(BF16)
    s_lo = (square - s_hi.astype(F32)).astype(BF16)
    ones = jnp.ones((8, width), BF16)
    s = contract(ones, contract(move, s_hi, 1, 0).astype(BF16), 1, 1)
    s += contract(ones, contract(move, s_lo, 1, 0).astype(BF16), 1, 1)
    fetch.wait()
    heads = gates.shape[1]
    local = heads // lax.axis_size("tp")
    pick_r, pick_c = iota((8, 2 * heads), 0), iota((8, 2 * heads), 1)
    want = ((pick_r & 3) // local) * heads + tp * local + (pick_r & (local - 1))
    pick = jnp.where(pick_c == want, 1.0, 0.0).astype(BF16)
    own_gates = contract(pick, gates[...].reshape(2 * heads, width), 1, 0).astype(BF16)
    g = contract(own_gates, scaled, 1, 1)

    def words(value, split):
        hi = value.astype(BF16).astype(F32)
        return jnp.where(iota(value.shape, 0) < split, hi, value - hi)

    g, s = words(g, 4), words(s, 1)
    lanes = iota((8, 128), 1)
    span = 128 // per
    for half in range(rows // 128):
        gh = g[:, half * 128 : (half + 1) * 128]
        sh = pltpu.roll(s[:, half * 128 : (half + 1) * 128], 64, 1)
        low = jnp.where(lanes < 64, gh, sh).astype(BF16)
        high = jnp.where(lanes < 64, sh, gh).astype(BF16)
        for k in range(span):
            out[half * span + k, block * per :, :] = low if k < span // 2 else high


def cell_kernel(accepted, stab, ib, fb, got, m0, n0, gated, kv_out, coef, *, features):
    z = lax.axis_index("kv")
    owners = got.shape[0]
    own, _, heads, dim, _ = m0.shape
    main = got.shape[1] - 8
    per = main // (4 * heads)
    props = per // own
    small = got[0, main:].astype(F32)
    for k in range(1, owners):
        small = small + got[k, main:].astype(F32)
    shift = (z & (128 // per - 1)) * per
    small = pltpu.roll(small, (128 - shift) & 127, 1)
    g = small + pltpu.roll(small, 4, 0)
    sq = pltpu.roll(small + pltpu.roll(small, 7, 0), 64, 1)
    packed = jnp.where(iota(g.shape, 0) < 4, g, pltpu.roll(sq, 4, 0))
    cols = packed.T[:per]
    inverse = lax.rsqrt(cols[:, 4:5] / features + EPSILON)
    col = iota((per, heads), 1)
    ibv, fbv = jnp.zeros((per, heads), F32), jnp.zeros((per, heads), F32)
    for h in range(heads):
        ibv, fbv = jnp.where(col == h, ib[h], ibv), jnp.where(col == h, fb[h], fbv)
    in_gate = cols[:, 0:2] * inverse + ibv
    f = cols[:, 2:4] * inverse + fbv
    log_forget = jnp.minimum(f, 0.0) - jnp.log1p(jnp.exp(-jnp.abs(f)))
    srow, scol = iota((own, heads), 0), iota((own, heads), 1)
    m = jnp.zeros((own, heads), F32)
    for b in range(own):
        for h in range(heads):
            m = jnp.where((srow == b) & (scol == h), stab[b, h, accepted[b]], m)
    stabs, retain, admit = [m], [], []
    for t in range(props):
        carried = log_forget[t * own : (t + 1) * own] + m
        incoming = in_gate[t * own : (t + 1) * own]
        top = jnp.maximum(carried, incoming)
        retain.append(jnp.exp(carried - top))
        admit.append(jnp.exp(incoming - top))
        m = top
        stabs.append(m)
    scale = dim ** (-0.5)
    factor = inverse * (1.0 / SHIFT)
    rr = iota((per, dim), 0) & (own - 1)

    def part(kind, h):
        rows = slice((kind * heads + h) * per, (kind * heads + h + 1) * per)
        total = decoded(got[0, rows])
        for k in range(1, owners):
            total = total + decoded(got[k, rows])
        return (total * factor).astype(BF16)

    outs = []
    for h in range(heads):
        q, k, v, o = part(0, h), part(1, h), part(2, h), part(3, h)
        kv_out[h] = k
        kv_out[heads + h] = v
        qf, kf, vf = q.astype(F32), k.astype(F32) * scale, v.astype(F32)
        base = jnp.zeros((per, dim), F32)
        for b in range(own):
            mine = jnp.where(rr == b, qf, 0.0).astype(BF16)
            mem = m0[b, 0, h]
            hi = mem.astype(BF16)
            lo = (mem - hi.astype(F32)).astype(BF16)
            base += contract(mine, hi, 1, 0) + contract(mine, lo, 1, 0)
        norm = n0[:, h, :]
        rows = []
        for t in range(props):
            sl = slice(t * own, (t + 1) * own)
            norm = retain[t][:, h : h + 1] * norm + admit[t][:, h : h + 1] * kf[sl]
            den = jnp.sum(qf[sl] * norm, -1, keepdims=True)
            weight = jnp.ones((own, 1), F32)
            num = jnp.zeros((own, dim), F32)
            for s in range(t, -1, -1):
                ss = slice(s * own, (s + 1) * own)
                dots = jnp.sum(qf[sl] * kf[ss], -1, keepdims=True)
                num += (weight * admit[s][:, h : h + 1] * dots) * vf[ss]
                weight = weight * retain[s][:, h : h + 1]
            num += weight * base[sl]
            floor = jnp.exp(-stabs[t + 1][:, h : h + 1])
            rows.append(num / jnp.maximum(jnp.abs(den), floor))
        hidden = jnp.concatenate(rows, 0)
        outs.append(jax.nn.sigmoid(o.astype(F32)) * hidden)
    both = jnp.concatenate(outs, 1).astype(BF16)
    for k in range(gated.shape[0]):
        gated[k] = both
    for t in range(props + 1):
        last = t - 1 if t else 0
        coef[t] = jnp.concatenate([stabs[t], retain[last], admit[last]], 1)


def memory_kernel(accepted, coef, m0, n0, kv, new_m, new_n, new_s, *, heads):
    b = pl.program_id(0)
    _, steps, _, dim, _ = new_m.shape
    per = kv.shape[1]
    props = steps - 1
    own = per // props
    scale = dim ** (-0.5)
    row, col = iota((heads, steps), 0), iota((heads, steps), 1)
    stabs = jnp.zeros((heads, steps), F32)
    for h in range(heads):
        for t in range(steps):
            stabs = jnp.where((row == h) & (col == t), coef[t, b, h], stabs)
        key = kv[h].astype(F32) * scale
        value = kv[heads + h].astype(F32)
        memory, norm = m0[0, 0, h], n0[0, 0, h : h + 1]
        new_m[0, 0, h] = memory
        new_n[0, 0, h : h + 1] = norm
        row_at = iota((per, dim), 0)
        keys = key.T
        lane = iota(keys.shape, 1)
        for t in range(props):
            keep, add = coef[t + 1, b, heads + h], coef[t + 1, b, 2 * heads + h]
            at = t * own + b
            vrow = jnp.sum(jnp.where(row_at == at, value, 0.0), 0, keepdims=True)
            krow = jnp.sum(jnp.where(row_at == at, key, 0.0), 0, keepdims=True)
            kcol = jnp.sum(jnp.where(lane == at, keys, 0.0), 1, keepdims=True)
            memory = keep * memory + (add * kcol) * vrow
            norm = keep * norm + add * krow
            new_m[0, t + 1, h] = memory
            new_n[0, t + 1, h : h + 1] = norm
    new_s[0] = stabs


def mix_kernel(gathered, w, after, out):
    owners, per, _ = gathered.shape
    rows = owners * per
    y = contract(w[...], gathered[...].reshape(rows, gathered.shape[2]), 0, 1).astype(BF16)
    out[...] = y.reshape(out.shape)


def finish_kernel(got, out, *, owners):
    total = got[0].astype(F32)
    for k in range(1, got.shape[0]):
        total = total + got[k].astype(F32)
    props, _, seqs = out.shape
    rows = props * seqs
    per = rows // owners
    own = per // props
    r, c = iota((rows, rows), 0), iota((rows, rows), 1)
    t, rest = c >> log2(seqs), c & (seqs - 1)
    source = (rest >> log2(own)) * per + t * own + (rest & (own - 1))
    move = jnp.where(r == source, 1.0, 0.0).astype(BF16)
    y = contract(total.astype(BF16), move, 1, 0).astype(BF16)
    for t in range(props):
        out[t] = y[:, t * seqs : (t + 1) * seqs]


def log2(n):
    assert n & (n - 1) == 0
    return n.bit_length() - 1


SMEM = pl.BlockSpec(memory_space=pltpu.SMEM)
VMEM = pl.BlockSpec(memory_space=pltpu.VMEM)


def held(shape, dtype):
    return pltpu.VMEM(shape, dtype)


def near(x):
    return pltpu.with_memory_space_constraint(x, pltpu.VMEM)


def local(
    tokens,
    norm_gain,
    w_query,
    w_key,
    w_value,
    w_outgate,
    gate_weight,
    input_bias,
    forget_bias,
    w_out,
    saved_memory,
    saved_normalizer,
    saved_stabilizer,
    accepted,
):
    owners, peers = lax.axis_size("kv"), lax.axis_size("tp")
    seqs, props, width = tokens.shape
    heads = input_bias.shape[0]
    own, saved, _, dim, _ = saved_memory.shape
    columns = w_query.shape[1]
    per = own * props
    blocks = 4 * columns // 128
    gates = gate_weight.transpose(0, 2, 1)
    all_heads = gates.shape[1]

    def whole(shape):
        return pl.BlockSpec(shape, lambda *_: (0,) * len(shape))

    send = pl.pallas_call(
        functools.partial(project_kernel, owners=owners),
        in_specs=[VMEM] * 6 + [pl.BlockSpec(memory_space=pl.ANY)],
        out_specs=[VMEM],
        out_shape=[held((owners, blocks * per + 8, 128), BF16)],
        scratch_shapes=[pltpu.VMEM((2, all_heads, width), BF16), pltpu.SemaphoreType.DMA],
        name="project",
    )(tokens, norm_gain.reshape(-1, 128), w_query, w_key, w_value, w_outgate, gates)[0]

    got = lax.all_to_all(send, "kv", split_axis=0, concat_axis=0, tiled=True)

    n0 = jnp.take_along_axis(saved_normalizer, accepted[:, None, None, None], 1)[:, 0]
    m0 = jnp.take_along_axis(saved_memory, accepted[:, None, None, None, None], 1)
    stab = saved_stabilizer.transpose(0, 2, 1)
    steps = props + 1
    gated, kv, coef = pl.pallas_call(
        functools.partial(cell_kernel, features=float(owners * width)),
        in_specs=[SMEM] * 4 + [VMEM] * 3,
        out_specs=[VMEM] * 3,
        out_shape=[
            held((owners, per, columns), BF16),
            held((2 * heads, per, dim), BF16),
            jax.ShapeDtypeStruct((steps, own, 3 * heads), F32),
        ],
        name="cell",
    )(accepted, stab, input_bias, forget_bias, near(got), near(m0), near(n0))

    gathered = lax.all_to_all(gated, "kv", split_axis=0, concat_axis=0, tiled=True)

    new_memory, new_n, new_s = pl.pallas_call(
        functools.partial(memory_kernel, heads=heads),
        grid_spec=pltpu.PrefetchScalarGridSpec(
            num_scalar_prefetch=1,
            grid=(own,),
            in_specs=[
                SMEM,
                pl.BlockSpec((1, 1, heads, dim, dim), lambda b, a: (b, a[b], 0, 0, 0)),
                pl.BlockSpec((1, 1, heads, dim), lambda b, a: (b, a[b], 0, 0)),
                whole((2 * heads, per, dim)),
            ],
            out_specs=[
                pl.BlockSpec((1, steps, heads, dim, dim), lambda b, a: (b, 0, 0, 0, 0)),
                pl.BlockSpec((1, steps, heads, dim), lambda b, a: (b, 0, 0, 0)),
                pl.BlockSpec((1, heads, steps), lambda b, a: (b, 0, 0)),
            ],
        ),
        out_shape=[
            jax.ShapeDtypeStruct((own, steps, heads, dim, dim), F32),
            jax.ShapeDtypeStruct((own, steps, heads, dim), F32),
            jax.ShapeDtypeStruct((own, heads, steps), F32),
        ],
        cost_estimate=pl.CostEstimate(flops=20_000_000, bytes_accessed=3_200_000, transcendentals=0),
        name="memory",
    )(accepted, coef, saved_memory, saved_normalizer, near(kv))

    terms = pl.pallas_call(
        mix_kernel,
        in_specs=[VMEM] * 2 + [pl.BlockSpec(memory_space=pl.ANY)],
        out_specs=[VMEM],
        out_shape=[held((peers, w_out.shape[1] // peers, seqs * props), BF16)],
        name="mix",
    )(near(gathered), near(w_out), new_s)[0]
    arrived = lax.all_to_all(terms, "tp", split_axis=0, concat_axis=0, tiled=True)

    mixed = pl.pallas_call(
        functools.partial(finish_kernel, owners=owners),
        in_specs=[VMEM],
        out_specs=VMEM,
        out_shape=jax.ShapeDtypeStruct((props, w_out.shape[1] // peers, seqs), BF16),
        name="finish",
    )(near(arrived))
    return mixed.transpose(2, 0, 1), new_memory, new_n, new_s.transpose(0, 2, 1)


def solution(mesh):
    return jax.shard_map(
        local,
        mesh=mesh,
        in_specs=(
            P("grp", None, "kv"),
            P(),
            P("kv", "tp"),
            P("kv", "tp"),
            P("kv", "tp"),
            P("kv", "tp"),
            P(),
            P("tp"),
            P("tp"),
            P("tp", "kv"),
            P(("grp", "kv"), None, "tp", None, None),
            P(("grp", "kv"), None, "tp", None),
            P(("grp", "kv"), None, "tp"),
            P(("grp", "kv")),
        ),
        out_specs=(
            P("grp", None, ("kv", "tp")),
            P(("grp", "kv"), None, "tp", None, None),
            P(("grp", "kv"), None, "tp", None),
            P(("grp", "kv"), None, "tp"),
        ),
        check_vma=False,
    )
```

```python
import functools

import jax
import jax.numpy as jnp
from jax import lax
from jax.experimental import pallas as pl
from jax.experimental.pallas import tpu as pltpu
from jax.sharding import PartitionSpec as P

EPSILON = 1e-06
F32 = jnp.float32
BF16 = jnp.bfloat16
SHIFT = 2.0**20


def iota(shape, dim):
    return lax.broadcasted_iota(jnp.int32, shape, dim)


def contract(a, b, da, db):
    return lax.dot_general(a, b, (((da,), (db,)), ((), ())), preferred_element_type=F32)


def coded(x):
    y = x * SHIFT
    return ((y * jnp.abs(y)) * (y * y)).astype(BF16)


def decoded(y):
    y = y.astype(F32)
    root = lax.rsqrt(lax.rsqrt(jnp.maximum(jnp.abs(y), 1e-37)))
    return jnp.where(y < 0.0, -root, root)


def project_kernel(tokens, gain, wq, wk, wv, wo, gates_hbm, up, down, keep_up, keep_down, small, gates, sem, *, owners):
    z, tp = lax.axis_index("kv"), lax.axis_index("tp")
    seqs, props, width = tokens.shape
    fetch = pltpu.make_async_copy(gates_hbm.at[:, :, pl.ds(pl.multiple_of(z * width, width), width)], gates, sem)
    fetch.start()
    rows = seqs * props
    per = rows // owners
    own = per // props
    x = tokens[...].astype(F32).reshape(rows, width)
    gain_rows = gain[...].astype(F32)
    pieces = []
    for j in range(width // 128):
        hit = iota(gain_rows.shape, 0) == z * (width // 128) + j
        pieces.append(jnp.sum(jnp.where(hit, gain_rows, 0.0), 0, keepdims=True))
    scaled = (x * jnp.concatenate(pieces, 1)).astype(BF16)
    r, c = iota((rows, rows), 0), iota((rows, rows), 1)
    source = (r & -per) + (r & (own - 1)) * props + ((r & (per - 1)) >> log2(own))
    move = jnp.where(c == source, 1.0, 0.0).astype(BF16)
    scaled = contract(move, scaled, 1, 0).astype(BF16)
    even = (z & 1) == 0

    def blocked(y):
        return [y[:, h * 128 : (h + 1) * 128].reshape(owners, per, 128) for h in range(y.shape[1] // 128)]

    for first, second, given, kept in ((wq, wk, up, keep_up), (wv, wo, down, keep_down)):
        theirs = jnp.where(even, second[...], first[...])
        ours = jnp.where(even, first[...], second[...])
        for h, y in enumerate(blocked(coded(contract(scaled, theirs, 1, 0)))):
            given[:, h * per : (h + 1) * per, :] = y
        for h, y in enumerate(blocked(contract(scaled, ours, 1, 0))):
            kept[:, h * per : (h + 1) * per, :] = y
    square = x * x
    s_hi = square.astype(BF16)
    s_lo = (square - s_hi.astype(F32)).astype(BF16)
    ones = jnp.ones((8, width), BF16)
    s = contract(ones, contract(move, s_hi, 1, 0).astype(BF16), 1, 1)
    s += contract(ones, contract(move, s_lo, 1, 0).astype(BF16), 1, 1)
    fetch.wait()
    heads = gates.shape[1]
    local = heads // lax.axis_size("tp")
    pick_r, pick_c = iota((8, 2 * heads), 0), iota((8, 2 * heads), 1)
    want = ((pick_r & 3) // local) * heads + tp * local + (pick_r & (local - 1))
    pick = jnp.where(pick_c == want, 1.0, 0.0).astype(BF16)
    own_gates = contract(pick, gates[...].reshape(2 * heads, width), 1, 0).astype(BF16)
    g = contract(own_gates, scaled, 1, 1)

    def words(value, split):
        hi = value.astype(BF16).astype(F32)
        return jnp.where(iota(value.shape, 0) < split, hi, value - hi)

    g, s = words(g, 4), words(s, 1)
    lanes = iota((8, 128), 1)
    span = 128 // per
    for half in range(rows // 128):
        gh = g[:, half * 128 : (half + 1) * 128]
        sh = pltpu.roll(s[:, half * 128 : (half + 1) * 128], 64, 1)
        low = jnp.where(lanes < 64, gh, sh).astype(BF16)
        high = jnp.where(lanes < 64, sh, gh).astype(BF16)
        for k in range(span):
            small[half * span + k] = low if k < span // 2 else high


def merge_kernel(got_up, got_down, keep_up, keep_down, small, out):
    half = got_up.shape[1]
    for at, got, kept in ((0, got_up, keep_up), (half, got_down, keep_down)):
        out[:, at : at + half, :] = coded(kept[...] + decoded(got[...]) * (1.0 / SHIFT))
    out[:, 2 * half :, :] = small[...]


def cell_kernel(accepted, stab, ib, fb, got, m0, n0, gated, kv_out, coef, *, features):
    z = lax.axis_index("kv")
    owners = got.shape[0]
    own, _, heads, dim, _ = m0.shape
    main = got.shape[1] - 8
    per = main // (2 * heads)
    props = per // own
    small = got[0, main:].astype(F32)
    for k in range(1, owners):
        small = small + got[k, main:].astype(F32)
    shift = (z & (128 // per - 1)) * per
    small = pltpu.roll(small, (128 - shift) & 127, 1)
    g = small + pltpu.roll(small, 4, 0)
    sq = pltpu.roll(small + pltpu.roll(small, 7, 0), 64, 1)
    packed = jnp.where(iota(g.shape, 0) < 4, g, pltpu.roll(sq, 4, 0))
    cols = packed.T[:per]
    inverse = lax.rsqrt(cols[:, 4:5] / features + EPSILON)
    col = iota((per, heads), 1)
    ibv, fbv = jnp.zeros((per, heads), F32), jnp.zeros((per, heads), F32)
    for h in range(heads):
        ibv, fbv = jnp.where(col == h, ib[h], ibv), jnp.where(col == h, fb[h], fbv)
    in_gate = cols[:, 0:2] * inverse + ibv
    f = cols[:, 2:4] * inverse + fbv
    log_forget = jnp.minimum(f, 0.0) - jnp.log1p(jnp.exp(-jnp.abs(f)))
    srow, scol = iota((own, heads), 0), iota((own, heads), 1)
    m = jnp.zeros((own, heads), F32)
    for b in range(own):
        for h in range(heads):
            m = jnp.where((srow == b) & (scol == h), stab[b, h, accepted[b]], m)
    stabs, retain, admit = [m], [], []
    for t in range(props):
        carried = log_forget[t * own : (t + 1) * own] + m
        incoming = in_gate[t * own : (t + 1) * own]
        top = jnp.maximum(carried, incoming)
        retain.append(jnp.exp(carried - top))
        admit.append(jnp.exp(incoming - top))
        m = top
        stabs.append(m)
    scale = dim ** (-0.5)
    factor = inverse * (1.0 / SHIFT)
    rr = iota((per, dim), 0) & (own - 1)

    def part(kind, h):
        at = ((kind >> 1) * heads + h) * per
        total = decoded(got[kind & 1, at : at + per])
        for k in range(2 + (kind & 1), owners, 2):
            total = total + decoded(got[k, at : at + per])
        return (total * factor).astype(BF16)

    outs = []
    for h in range(heads):
        q, k, v, o = part(0, h), part(1, h), part(2, h), part(3, h)
        kv_out[h] = k
        kv_out[heads + h] = v
        qf, kf, vf = q.astype(F32), k.astype(F32) * scale, v.astype(F32)
        base = jnp.zeros((per, dim), F32)
        for b in range(own):
            mine = jnp.where(rr == b, qf, 0.0).astype(BF16)
            mem = m0[b, 0, h]
            hi = mem.astype(BF16)
            lo = (mem - hi.astype(F32)).astype(BF16)
            base += contract(mine, hi, 1, 0) + contract(mine, lo, 1, 0)
        norm = n0[:, h, :]
        rows = []
        for t in range(props):
            sl = slice(t * own, (t + 1) * own)
            norm = retain[t][:, h : h + 1] * norm + admit[t][:, h : h + 1] * kf[sl]
            den = jnp.sum(qf[sl] * norm, -1, keepdims=True)
            weight = jnp.ones((own, 1), F32)
            num = jnp.zeros((own, dim), F32)
            for s in range(t, -1, -1):
                ss = slice(s * own, (s + 1) * own)
                dots = jnp.sum(qf[sl] * kf[ss], -1, keepdims=True)
                num += (weight * admit[s][:, h : h + 1] * dots) * vf[ss]
                weight = weight * retain[s][:, h : h + 1]
            num += weight * base[sl]
            floor = jnp.exp(-stabs[t + 1][:, h : h + 1])
            rows.append(num / jnp.maximum(jnp.abs(den), floor))
        hidden = jnp.concatenate(rows, 0)
        outs.append(jax.nn.sigmoid(o.astype(F32)) * hidden)
    both = jnp.concatenate(outs, 1).astype(BF16)
    for k in range(gated.shape[0]):
        gated[k] = both
    for t in range(props + 1):
        last = t - 1 if t else 0
        coef[t] = jnp.concatenate([stabs[t], retain[last], admit[last]], 1)


def memory_kernel(accepted, coef, m0, n0, kv, new_m, new_n, new_s, *, heads):
    b = pl.program_id(0)
    _, steps, _, dim, _ = new_m.shape
    per = kv.shape[1]
    props = steps - 1
    own = per // props
    scale = dim ** (-0.5)
    row, col = iota((heads, steps), 0), iota((heads, steps), 1)
    stabs = jnp.zeros((heads, steps), F32)
    for h in range(heads):
        for t in range(steps):
            stabs = jnp.where((row == h) & (col == t), coef[t, b, h], stabs)
        key = kv[h].astype(F32) * scale
        value = kv[heads + h].astype(F32)
        memory, norm = m0[0, 0, h], n0[0, 0, h : h + 1]
        new_m[0, 0, h] = memory
        new_n[0, 0, h : h + 1] = norm
        row_at = iota((per, dim), 0)
        keys = key.T
        lane = iota(keys.shape, 1)
        for t in range(props):
            keep, add = coef[t + 1, b, heads + h], coef[t + 1, b, 2 * heads + h]
            at = t * own + b
            vrow = jnp.sum(jnp.where(row_at == at, value, 0.0), 0, keepdims=True)
            krow = jnp.sum(jnp.where(row_at == at, key, 0.0), 0, keepdims=True)
            kcol = jnp.sum(jnp.where(lane == at, keys, 0.0), 1, keepdims=True)
            memory = keep * memory + (add * kcol) * vrow
            norm = keep * norm + add * krow
            new_m[0, t + 1, h] = memory
            new_n[0, t + 1, h : h + 1] = norm
    new_s[0] = stabs


def mix_kernel(gathered, w, after, out):
    owners, per, _ = gathered.shape
    rows = owners * per
    y = contract(w[...], gathered[...].reshape(rows, gathered.shape[2]), 0, 1).astype(BF16)
    out[...] = y.reshape(out.shape)


def finish_kernel(got, out, *, owners):
    total = got[0].astype(F32)
    for k in range(1, got.shape[0]):
        total = total + got[k].astype(F32)
    props, _, seqs = out.shape
    rows = props * seqs
    per = rows // owners
    own = per // props
    r, c = iota((rows, rows), 0), iota((rows, rows), 1)
    t, rest = c >> log2(seqs), c & (seqs - 1)
    source = (rest >> log2(own)) * per + t * own + (rest & (own - 1))
    move = jnp.where(r == source, 1.0, 0.0).astype(BF16)
    y = contract(total.astype(BF16), move, 1, 0).astype(BF16)
    for t in range(props):
        out[t] = y[:, t * seqs : (t + 1) * seqs]


def log2(n):
    assert n & (n - 1) == 0
    return n.bit_length() - 1


SMEM = pl.BlockSpec(memory_space=pltpu.SMEM)
VMEM = pl.BlockSpec(memory_space=pltpu.VMEM)


def held(shape, dtype):
    return pltpu.VMEM(shape, dtype)


def near(x):
    return pltpu.with_memory_space_constraint(x, pltpu.VMEM)


def local(
    tokens,
    norm_gain,
    w_query,
    w_key,
    w_value,
    w_outgate,
    gate_weight,
    input_bias,
    forget_bias,
    w_out,
    saved_memory,
    saved_normalizer,
    saved_stabilizer,
    accepted,
):
    owners, peers = lax.axis_size("kv"), lax.axis_size("tp")
    seqs, props, width = tokens.shape
    heads = input_bias.shape[0]
    own, saved, _, dim, _ = saved_memory.shape
    columns = w_query.shape[1]
    per = own * props
    gates = gate_weight.transpose(0, 2, 1)
    all_heads = gates.shape[1]

    def whole(shape):
        return pl.BlockSpec(shape, lambda *_: (0,) * len(shape))

    half = columns // 128 * per
    up, down, keep_up, keep_down, small = pl.pallas_call(
        functools.partial(project_kernel, owners=owners),
        in_specs=[VMEM] * 6 + [pl.BlockSpec(memory_space=pl.ANY)],
        out_specs=[VMEM] * 5,
        out_shape=[
            held((owners, half, 128), BF16),
            held((owners, half, 128), BF16),
            held((owners, half, 128), F32),
            held((owners, half, 128), F32),
            held((owners, 8, 128), BF16),
        ],
        scratch_shapes=[pltpu.VMEM((2, all_heads, width), BF16), pltpu.SemaphoreType.DMA],
        name="project",
    )(tokens, norm_gain.reshape(-1, 128), w_query, w_key, w_value, w_outgate, gates)

    with_next = [(i, i ^ 1) for i in range(owners)]
    with_last = [(i, (((i + 1) ^ 1) - 1) % owners) for i in range(owners)]
    got_up = lax.ppermute(up, "kv", with_next)
    got_down = lax.ppermute(down, "kv", with_last)
    send = pl.pallas_call(
        merge_kernel,
        in_specs=[VMEM] * 5,
        out_specs=[VMEM],
        out_shape=[held((owners, 2 * half + 8, 128), BF16)],
        name="merge",
    )(near(got_up), near(got_down), near(keep_up), near(keep_down), near(small))[0]

    got = lax.all_to_all(send, "kv", split_axis=0, concat_axis=0, tiled=True)

    n0 = jnp.take_along_axis(saved_normalizer, accepted[:, None, None, None], 1)[:, 0]
    m0 = jnp.take_along_axis(saved_memory, accepted[:, None, None, None, None], 1)
    stab = saved_stabilizer.transpose(0, 2, 1)
    steps = props + 1
    gated, kv, coef = pl.pallas_call(
        functools.partial(cell_kernel, features=float(owners * width)),
        in_specs=[SMEM] * 4 + [VMEM] * 3,
        out_specs=[VMEM] * 3,
        out_shape=[
            held((owners, per, columns), BF16),
            held((2 * heads, per, dim), BF16),
            jax.ShapeDtypeStruct((steps, own, 3 * heads), F32),
        ],
        name="cell",
    )(accepted, stab, input_bias, forget_bias, near(got), near(m0), near(n0))

    gathered = lax.all_to_all(gated, "kv", split_axis=0, concat_axis=0, tiled=True)

    new_memory, new_n, new_s = pl.pallas_call(
        functools.partial(memory_kernel, heads=heads),
        grid_spec=pltpu.PrefetchScalarGridSpec(
            num_scalar_prefetch=1,
            grid=(own,),
            in_specs=[
                SMEM,
                pl.BlockSpec((1, 1, heads, dim, dim), lambda b, a: (b, a[b], 0, 0, 0)),
                pl.BlockSpec((1, 1, heads, dim), lambda b, a: (b, a[b], 0, 0)),
                whole((2 * heads, per, dim)),
            ],
            out_specs=[
                pl.BlockSpec((1, steps, heads, dim, dim), lambda b, a: (b, 0, 0, 0, 0)),
                pl.BlockSpec((1, steps, heads, dim), lambda b, a: (b, 0, 0, 0)),
                pl.BlockSpec((1, heads, steps), lambda b, a: (b, 0, 0)),
            ],
        ),
        out_shape=[
            jax.ShapeDtypeStruct((own, steps, heads, dim, dim), F32),
            jax.ShapeDtypeStruct((own, steps, heads, dim), F32),
            jax.ShapeDtypeStruct((own, heads, steps), F32),
        ],
        cost_estimate=pl.CostEstimate(flops=20_000_000, bytes_accessed=3_200_000, transcendentals=0),
        name="memory",
    )(accepted, coef, saved_memory, saved_normalizer, near(kv))

    terms = pl.pallas_call(
        mix_kernel,
        in_specs=[VMEM] * 2 + [pl.BlockSpec(memory_space=pl.ANY)],
        out_specs=[VMEM],
        out_shape=[held((peers, w_out.shape[1] // peers, seqs * props), BF16)],
        name="mix",
    )(near(gathered), near(w_out), new_s)[0]
    arrived = lax.all_to_all(terms, "tp", split_axis=0, concat_axis=0, tiled=True)

    mixed = pl.pallas_call(
        functools.partial(finish_kernel, owners=owners),
        in_specs=[VMEM],
        out_specs=VMEM,
        out_shape=jax.ShapeDtypeStruct((props, w_out.shape[1] // peers, seqs), BF16),
        name="finish",
    )(near(arrived))
    return mixed.transpose(2, 0, 1), new_memory, new_n, new_s.transpose(0, 2, 1)


def solution(mesh):
    return jax.shard_map(
        local,
        mesh=mesh,
        in_specs=(
            P("grp", None, "kv"),
            P(),
            P("kv", "tp"),
            P("kv", "tp"),
            P("kv", "tp"),
            P("kv", "tp"),
            P(),
            P("tp"),
            P("tp"),
            P("tp", "kv"),
            P(("grp", "kv"), None, "tp", None, None),
            P(("grp", "kv"), None, "tp", None),
            P(("grp", "kv"), None, "tp"),
            P(("grp", "kv")),
        ),
        out_specs=(
            P("grp", None, ("kv", "tp")),
            P(("grp", "kv"), None, "tp", None, None),
            P(("grp", "kv"), None, "tp", None),
            P(("grp", "kv"), None, "tp"),
        ),
        check_vma=False,
    )
```

```python
import functools

import jax
import jax.numpy as jnp
from jax import lax
from jax.experimental import pallas as pl
from jax.experimental.pallas import tpu as pltpu
from jax.sharding import PartitionSpec as P

EPSILON = 1e-06
F32 = jnp.float32
BF16 = jnp.bfloat16
SHIFT = 2.0**20
TURN = ((1, 1, 0), (1, 1, 8))


def iota(shape, dim):
    return lax.broadcasted_iota(jnp.int32, shape, dim)


def contract(a, b, da, db):
    return lax.dot_general(a, b, (((da,), (db,)), ((), ())), preferred_element_type=F32)


def coded(x):
    y = x * SHIFT
    return ((y * jnp.abs(y)) * (y * y)).astype(BF16)


def decoded(y):
    y = y.astype(F32)
    root = lax.rsqrt(lax.rsqrt(jnp.maximum(jnp.abs(y), 1e-37)))
    return jnp.where(y < 0.0, -root, root)


def moved_rows(rows, per, own):
    r, c = iota((rows, rows), 0), iota((rows, rows), 1)
    stride, _, start = TURN[0]
    place = ((r & -per) * stride + start * per) & (rows - 1)
    source = place + (r & (own - 1)) * (per // own) + ((r & (per - 1)) >> log2(own))
    return jnp.where(c == source, 1.0, 0.0).astype(BF16)


def blocked(y, owners):
    return [y[:, h * 128 : (h + 1) * 128].reshape(owners, -1, 128) for h in range(y.shape[1] // 128)]


def give_kernel(tokens, gain, wq, wk, wv, wo, up, down, scaled_out, *, owners):
    z = lax.axis_index("kv")
    seqs, props, width = tokens.shape
    rows = seqs * props
    per = rows // owners
    own = per // props
    x = tokens[...].astype(F32).reshape(rows, width)
    gain_rows = gain[...].astype(F32)
    pieces = []
    for j in range(width // 128):
        hit = iota(gain_rows.shape, 0) == z * (width // 128) + j
        pieces.append(jnp.sum(jnp.where(hit, gain_rows, 0.0), 0, keepdims=True))
    scaled = (x * jnp.concatenate(pieces, 1)).astype(BF16)
    scaled = contract(moved_rows(rows, per, own), scaled, 1, 0).astype(BF16)
    scaled_out[...] = scaled
    even = (z & 1) == 0
    for first, second, given in ((wq, wk, up), (wv, wo, down)):
        theirs = jnp.where(even, second[...], first[...])
        for h, y in enumerate(blocked(coded(contract(scaled, theirs, 1, 0)), owners)):
            given[:, h * per : (h + 1) * per, :] = y


def keep_kernel(tokens, scaled_in, wq, wk, wv, wo, gates_hbm, keep_up, keep_down, small, gates, sem, *, owners):
    z, tp = lax.axis_index("kv"), lax.axis_index("tp")
    seqs, props, width = tokens.shape
    fetch = pltpu.make_async_copy(gates_hbm.at[:, :, pl.ds(pl.multiple_of(z * width, width), width)], gates, sem)
    fetch.start()
    rows = seqs * props
    per = rows // owners
    own = per // props
    x = tokens[...].astype(F32).reshape(rows, width)
    scaled = scaled_in[...]
    even = (z & 1) == 0
    for first, second, kept in ((wq, wk, keep_up), (wv, wo, keep_down)):
        ours = jnp.where(even, first[...], second[...])
        for h, y in enumerate(blocked(contract(scaled, ours, 1, 0), owners)):
            kept[:, h * per : (h + 1) * per, :] = y
    move = moved_rows(rows, per, own)
    square = x * x
    s_hi = square.astype(BF16)
    s_lo = (square - s_hi.astype(F32)).astype(BF16)
    ones = jnp.ones((8, width), BF16)
    s = contract(ones, contract(move, s_hi, 1, 0).astype(BF16), 1, 1)
    s += contract(ones, contract(move, s_lo, 1, 0).astype(BF16), 1, 1)
    fetch.wait()
    heads = gates.shape[1]
    local = heads // lax.axis_size("tp")
    pick_r, pick_c = iota((8, 2 * heads), 0), iota((8, 2 * heads), 1)
    want = ((pick_r & 3) // local) * heads + tp * local + (pick_r & (local - 1))
    pick = jnp.where(pick_c == want, 1.0, 0.0).astype(BF16)
    own_gates = contract(pick, gates[...].reshape(2 * heads, width), 1, 0).astype(BF16)
    g = contract(own_gates, scaled, 1, 1)

    def words(value, split):
        hi = value.astype(BF16).astype(F32)
        return jnp.where(iota(value.shape, 0) < split, hi, value - hi)

    g, s = words(g, 4), words(s, 1)
    lanes = iota((8, 128), 1)
    span = 128 // per
    for half in range(rows // 128):
        gh = g[:, half * 128 : (half + 1) * 128]
        sh = pltpu.roll(s[:, half * 128 : (half + 1) * 128], 64, 1)
        low = jnp.where(lanes < 64, gh, sh).astype(BF16)
        high = jnp.where(lanes < 64, sh, gh).astype(BF16)
        for k in range(span):
            small[half * span + k] = low if k < span // 2 else high


def merge_kernel(got_up, got_down, keep_up, keep_down, small, out, made, sems):
    owners, half, _ = got_up.shape
    quarter = owners // 4
    copies = []
    for part in range(4):
        own = slice(part * quarter, (part + 1) * quarter)
        for at, got, kept in ((0, got_up, keep_up), (half, got_down, keep_down)):
            made[own, at : at + half, :] = coded(kept[own] + decoded(got[own]) * (1.0 / SHIFT))
        made[own, 2 * half :, :] = small[own]
        copies.append(pltpu.make_async_copy(made.at[own], out.at[own], sems.at[part]))
        copies[part].start()
    for copy in copies:
        copy.wait()


def take_kernel(accepted, stab, ib, fb, memory_hbm, norms, m0, n0, words, move, bias, first, sems, *, owners, seqs):
    own, _, heads, dim, _ = m0.shape
    copies = []
    for b in range(own):
        copies.append(pltpu.make_async_copy(memory_hbm.at[b, accepted[b]], m0.at[b, 0], sems.at[b]))
        copies[b].start()
    col = iota(bias.shape[1:], 1)
    for k, source in enumerate((ib, fb)):
        value = jnp.zeros(bias.shape[1:], F32)
        for h in range(heads):
            value = jnp.where(col == h, source[h], value)
        bias[k] = value
    srow, scol = iota((own, heads), 0), iota((own, heads), 1)
    m = jnp.zeros((own, heads), F32)
    for b in range(own):
        for h in range(heads):
            m = jnp.where((srow == b) & (scol == h), stab[b, h, accepted[b]], m)
    first[...] = m
    rows = move.shape[0]
    props = rows // seqs
    per = rows // owners
    r, c = iota((rows, rows), 0), iota((rows, rows), 1)
    t, rest = c >> log2(seqs), c & (seqs - 1)
    place = (((rest >> log2(own)) - TURN[1][2]) * TURN[1][1]) & (owners - 1)
    source = place * per + t * own + (rest & (own - 1))
    move[...] = jnp.where(r == source, 1.0, 0.0).astype(BF16)
    for b in range(own):
        n0[b] = norms[b, accepted[b]]
        copies[b].wait()
        for h in range(heads):
            value = m0[b, 0, h]
            hi = value.astype(BF16)
            words[h, b * dim : (b + 1) * dim, :dim] = hi
            words[h, b * dim : (b + 1) * dim, dim:] = (value - hi.astype(F32)).astype(BF16)


def cell_kernel(got, words, n0, bias, start, gated, kv_out, coef, *, features):
    z = lax.axis_index("kv")
    owners = got.shape[0]
    own, heads, dim = n0.shape
    main = got.shape[1] - 8
    per = main // (2 * heads)
    props = per // own
    small = got[0, main:].astype(F32)
    for k in range(1, owners):
        small = small + got[k, main:].astype(F32)
    shift = (((z - TURN[0][2]) * TURN[0][1]) & (128 // per - 1)) * per
    small = pltpu.roll(small, (128 - shift) & 127, 1)
    g = small + pltpu.roll(small, 4, 0)
    sq = pltpu.roll(small + pltpu.roll(small, 7, 0), 64, 1)
    packed = jnp.where(iota(g.shape, 0) < 4, g, pltpu.roll(sq, 4, 0))
    cols = packed.T[:per]
    inverse = lax.rsqrt(cols[:, 4:5] / features + EPSILON)
    in_gate = cols[:, 0:2] * inverse + bias[0]
    f = cols[:, 2:4] * inverse + bias[1]
    log_forget = jnp.minimum(f, 0.0) - jnp.log1p(jnp.exp(-jnp.abs(f)))
    m = start[...]
    stabs, retain, admit = [m], [], []
    for t in range(props):
        carried = log_forget[t * own : (t + 1) * own] + m
        incoming = in_gate[t * own : (t + 1) * own]
        top = jnp.maximum(carried, incoming)
        retain.append(jnp.exp(carried - top))
        admit.append(jnp.exp(incoming - top))
        m = top
        stabs.append(m)
    scale = dim ** (-0.5)
    factor = inverse * (1.0 / SHIFT)
    rr = iota((per, dim), 0) & (own - 1)

    def part(kind, h):
        at = ((kind >> 1) * heads + h) * per
        first = (kind + TURN[0][2]) & 1
        total = decoded(got[first, at : at + per])
        for k in range(2 + first, owners, 2):
            total = total + decoded(got[k, at : at + per])
        return (total * factor).astype(BF16)

    outs = []
    for h in range(heads):
        q, k, v, o = part(0, h), part(1, h), part(2, h), part(3, h)
        kv_out[h] = k
        kv_out[heads + h] = v
        qf, kf, vf = q.astype(F32), k.astype(F32) * scale, v.astype(F32)
        wide = jnp.concatenate([jnp.where(rr == b, qf, 0.0) for b in range(own)], 1).astype(BF16)
        both = contract(wide, words[h], 1, 0)
        base = both[:, :dim] + both[:, dim:]
        norm = n0[:, h, :]
        rows = []
        for t in range(props):
            sl = slice(t * own, (t + 1) * own)
            norm = retain[t][:, h : h + 1] * norm + admit[t][:, h : h + 1] * kf[sl]
            den = jnp.sum(qf[sl] * norm, -1, keepdims=True)
            weight = jnp.ones((own, 1), F32)
            num = jnp.zeros((own, dim), F32)
            for s in range(t, -1, -1):
                ss = slice(s * own, (s + 1) * own)
                dots = jnp.sum(qf[sl] * kf[ss], -1, keepdims=True)
                num += (weight * admit[s][:, h : h + 1] * dots) * vf[ss]
                weight = weight * retain[s][:, h : h + 1]
            num += weight * base[sl]
            floor = jnp.exp(-stabs[t + 1][:, h : h + 1])
            rows.append(num / jnp.maximum(jnp.abs(den), floor))
        hidden = jnp.concatenate(rows, 0)
        outs.append(jax.nn.sigmoid(o.astype(F32)) * hidden)
    result = jnp.concatenate(outs, 1).astype(BF16)
    for k in range(gated.shape[0]):
        gated[k] = result
    for t in range(props + 1):
        last = t - 1 if t else 0
        coef[t] = jnp.concatenate([stabs[t], retain[last], admit[last]], 1)


def memory_kernel(coef, m0, n0, kv, new_m, new_n, new_s, made, sems):
    own, _, heads, dim, _ = m0.shape
    per = kv.shape[1]
    props = per // own
    steps = props + 1
    scale = dim ** (-0.5)
    row, col = iota((heads, steps), 0), iota((heads, steps), 1)
    row_at = iota((per, dim), 0)
    sent = []

    def send(source, b, t):
        copy = pltpu.make_async_copy(source, new_m.at[b, t], sems.at[b, t])
        copy.start()
        sent.append(copy)

    for b in range(own):
        send(m0.at[b, 0], b, 0)
    for b in range(own):
        stabs = jnp.zeros((heads, steps), F32)
        norms = []
        for h in range(heads):
            norms.append(n0[b, h : h + 1])
            new_n[b, 0, h : h + 1] = norms[h]
            for t in range(steps):
                stabs = jnp.where((row == h) & (col == t), coef[t, b, h], stabs)
        new_s[b] = stabs
        memories = [m0[b, 0, h] for h in range(heads)]
        for t in range(props):
            for h in range(heads):
                keep, add = coef[t + 1, b, heads + h], coef[t + 1, b, 2 * heads + h] * scale
                one = jnp.where(row_at == t * own + b, kv[h].astype(F32), 0.0)
                memories[h] = keep * memories[h] + add * contract(one.astype(BF16), kv[heads + h], 0, 0)
                norms[h] = keep * norms[h] + add * jnp.sum(one, 0, keepdims=True)
                made[b, t, h] = memories[h]
                new_n[b, t + 1, h : h + 1] = norms[h]
            send(made.at[b, t], b, t + 1)
    for copy in sent:
        copy.wait()


def mix_kernel(gathered, w, after, out):
    owners, per, _ = gathered.shape
    rows = owners * per
    y = contract(w[...], gathered[...].reshape(rows, gathered.shape[2]), 0, 1).astype(BF16)
    out[...] = y.reshape(out.shape)


def finish_kernel(got, move, out):
    total = got[0].astype(F32)
    for k in range(1, got.shape[0]):
        total = total + got[k].astype(F32)
    props, _, seqs = out.shape
    y = contract(total.astype(BF16), move[...], 1, 0).astype(BF16)
    for t in range(props):
        out[t] = y[:, t * seqs : (t + 1) * seqs]


def log2(n):
    assert n & (n - 1) == 0
    return n.bit_length() - 1


SMEM = pl.BlockSpec(memory_space=pltpu.SMEM)
VMEM = pl.BlockSpec(memory_space=pltpu.VMEM)


def held(shape, dtype):
    return pltpu.VMEM(shape, dtype)


def near(x):
    return pltpu.with_memory_space_constraint(x, pltpu.VMEM)


def local(
    tokens,
    norm_gain,
    w_query,
    w_key,
    w_value,
    w_outgate,
    gate_weight,
    input_bias,
    forget_bias,
    w_out,
    saved_memory,
    saved_normalizer,
    saved_stabilizer,
    accepted,
):
    owners, peers = lax.axis_size("kv"), lax.axis_size("tp")
    seqs, props, width = tokens.shape
    heads = input_bias.shape[0]
    own, saved, _, dim, _ = saved_memory.shape
    columns = w_query.shape[1]
    per = own * props
    gates = gate_weight.transpose(0, 2, 1)
    all_heads = gates.shape[1]

    def whole(shape):
        return pl.BlockSpec(shape, lambda *_: (0,) * len(shape))

    half = columns // 128 * per
    weights = (w_query, w_key, w_value, w_outgate)
    up, down, scaled = pl.pallas_call(
        functools.partial(give_kernel, owners=owners),
        in_specs=[VMEM] * 6,
        out_specs=[VMEM] * 3,
        out_shape=[
            held((owners, half, 128), BF16),
            held((owners, half, 128), BF16),
            held((seqs * props, width), BF16),
        ],
        name="give",
    )(tokens, norm_gain.reshape(-1, 128), *weights)

    with_next = [(i, i ^ 1) for i in range(owners)]
    with_last = [(i, (((i + 1) ^ 1) - 1) % owners) for i in range(owners)]
    got_up = lax.ppermute(up, "kv", with_next)
    got_down = lax.ppermute(down, "kv", with_last)
    keep_up, keep_down, small = pl.pallas_call(
        functools.partial(keep_kernel, owners=owners),
        in_specs=[VMEM] * 6 + [pl.BlockSpec(memory_space=pl.ANY)],
        out_specs=[VMEM] * 3,
        out_shape=[
            held((owners, half, 128), F32),
            held((owners, half, 128), F32),
            held((owners, 8, 128), BF16),
        ],
        scratch_shapes=[pltpu.VMEM((2, all_heads, width), BF16), pltpu.SemaphoreType.DMA],
        cost_estimate=pl.CostEstimate(flops=80_000_000, bytes_accessed=1_000_000, transcendentals=0),
        name="keep",
    )(tokens, near(scaled), *weights, gates)
    send = pl.pallas_call(
        merge_kernel,
        in_specs=[VMEM] * 5,
        out_specs=[pl.BlockSpec(memory_space=pl.ANY)],
        out_shape=[jax.ShapeDtypeStruct((owners, 2 * half + 8, 128), BF16)],
        scratch_shapes=[pltpu.VMEM((owners, 2 * half + 8, 128), BF16), pltpu.SemaphoreType.DMA((4,))],
        name="merge",
    )(near(got_up), near(got_down), near(keep_up), near(keep_down), near(small))[0]

    turned = [[[(stride * k + start) % owners for k in range(owners)]] for stride, _, start in TURN]
    turned = [None if x[0] == list(range(owners)) else x for x in turned]
    got = lax.all_to_all(send, "kv", 0, 0, axis_index_groups=turned[0], tiled=True)

    stab = saved_stabilizer.transpose(0, 2, 1)
    m0, n0, words, move, bias, first = pl.pallas_call(
        functools.partial(take_kernel, owners=owners, seqs=seqs),
        in_specs=[SMEM] * 4 + [pl.BlockSpec(memory_space=pl.ANY), VMEM],
        out_specs=[VMEM] * 6,
        out_shape=[
            held((own, 1, heads, dim, dim), F32),
            held((own, heads, dim), F32),
            held((heads, own * dim, 2 * dim), BF16),
            held((seqs * props, seqs * props), BF16),
            held((2, per, heads), F32),
            held((own, heads), F32),
        ],
        scratch_shapes=[pltpu.SemaphoreType.DMA((own,))],
        cost_estimate=pl.CostEstimate(flops=40_000_000, bytes_accessed=1_000_000, transcendentals=0),
        name="take",
    )(accepted, stab, input_bias, forget_bias, saved_memory, saved_normalizer)
    steps = props + 1
    gated, kv, coef = pl.pallas_call(
        functools.partial(cell_kernel, features=float(owners * width)),
        in_specs=[VMEM] * 5,
        out_specs=[VMEM] * 3,
        out_shape=[
            held((owners, per, columns), BF16),
            held((2 * heads, per, dim), BF16),
            jax.ShapeDtypeStruct((steps, own, 3 * heads), F32),
        ],
        name="cell",
    )(near(got), near(words), near(n0), near(bias), near(first))

    gathered = lax.all_to_all(gated, "kv", 0, 0, axis_index_groups=turned[1], tiled=True)

    new_memory, new_n, new_s = pl.pallas_call(
        memory_kernel,
        in_specs=[SMEM] + [VMEM] * 3,
        out_specs=[pl.BlockSpec(memory_space=pl.ANY), VMEM, VMEM],
        out_shape=[
            jax.ShapeDtypeStruct((own, steps, heads, dim, dim), F32),
            jax.ShapeDtypeStruct((own, steps, heads, dim), F32),
            jax.ShapeDtypeStruct((own, heads, steps), F32),
        ],
        scratch_shapes=[pltpu.VMEM((own, props, heads, dim, dim), F32), pltpu.SemaphoreType.DMA((own, steps))],
        cost_estimate=pl.CostEstimate(flops=20_000_000, bytes_accessed=3_200_000, transcendentals=0),
        name="memory",
    )(coef, near(m0), near(n0), near(kv))

    terms = pl.pallas_call(
        mix_kernel,
        in_specs=[VMEM] * 2 + [pl.BlockSpec(memory_space=pl.ANY)],
        out_specs=[VMEM],
        out_shape=[held((peers, w_out.shape[1] // peers, seqs * props), BF16)],
        name="mix",
    )(near(gathered), near(w_out), new_s)[0]
    arrived = lax.all_to_all(terms, "tp", split_axis=0, concat_axis=0, tiled=True)

    mixed = pl.pallas_call(
        finish_kernel,
        in_specs=[VMEM] * 2,
        out_specs=VMEM,
        out_shape=jax.ShapeDtypeStruct((props, w_out.shape[1] // peers, seqs), BF16),
        name="finish",
    )(near(arrived), near(move))
    return mixed.transpose(2, 0, 1), new_memory, new_n, new_s.transpose(0, 2, 1)


def solution(mesh):
    return jax.shard_map(
        local,
        mesh=mesh,
        in_specs=(
            P("grp", None, "kv"),
            P(),
            P("kv", "tp"),
            P("kv", "tp"),
            P("kv", "tp"),
            P("kv", "tp"),
            P(),
            P("tp"),
            P("tp"),
            P("tp", "kv"),
            P(("grp", "kv"), None, "tp", None, None),
            P(("grp", "kv"), None, "tp", None),
            P(("grp", "kv"), None, "tp"),
            P(("grp", "kv")),
        ),
        out_specs=(
            P("grp", None, ("kv", "tp")),
            P(("grp", "kv"), None, "tp", None, None),
            P(("grp", "kv"), None, "tp", None),
            P(("grp", "kv"), None, "tp"),
        ),
        check_vma=False,
    )
```

```python
import functools

import jax
import jax.numpy as jnp
from jax import lax
from jax.experimental import pallas as pl
from jax.experimental.pallas import tpu as pltpu
from jax.sharding import PartitionSpec as P

EPSILON = 1e-06
F32 = jnp.float32
BF16 = jnp.bfloat16
SHIFT = 2.0**20
TURN = ((1, 1, 0), (1, 1, 8))


def iota(shape, dim):
    return lax.broadcasted_iota(jnp.int32, shape, dim)


def contract(a, b, da, db):
    return lax.dot_general(a, b, (((da,), (db,)), ((), ())), preferred_element_type=F32)


def coded(x):
    y = x * SHIFT
    return ((y * jnp.abs(y)) * (y * y)).astype(BF16)


def decoded(y):
    y = y.astype(F32)
    root = lax.rsqrt(lax.rsqrt(jnp.maximum(jnp.abs(y), 1e-37)))
    return jnp.where(y < 0.0, -root, root)


def moved_rows(rows, per, own):
    r, c = iota((rows, rows), 0), iota((rows, rows), 1)
    stride, _, start = TURN[0]
    place = ((r & -per) * stride + start * per) & (rows - 1)
    source = place + (r & (own - 1)) * (per // own) + ((r & (per - 1)) >> log2(own))
    return jnp.where(c == source, 1.0, 0.0).astype(BF16)


def blocked(y, owners):
    return [y[:, h * 128 : (h + 1) * 128].reshape(owners, -1, 128) for h in range(y.shape[1] // 128)]


def give_kernel(tokens, gain, wq, wk, wv, wo, up, down, scaled_out, theirs, sems, *, owners):
    z = lax.axis_index("kv")
    seqs, props, width = tokens.shape
    even = (z & 1) == 0
    copies = []
    for k, (first, second) in enumerate(((wq, wk), (wv, wo))):
        copies.append(pltpu.make_async_copy(second, theirs.at[k], sems.at[k]))
        other = pltpu.make_async_copy(first, theirs.at[k], sems.at[k])
        pl.when(even)(copies[k].start)
        pl.when(jnp.logical_not(even))(other.start)
    rows = seqs * props
    per = rows // owners
    own = per // props
    x = tokens[...].astype(F32).reshape(rows, width)
    gain_rows = gain[...].astype(F32)
    pieces = []
    for j in range(width // 128):
        hit = iota(gain_rows.shape, 0) == z * (width // 128) + j
        pieces.append(jnp.sum(jnp.where(hit, gain_rows, 0.0), 0, keepdims=True))
    scaled = (x * jnp.concatenate(pieces, 1)).astype(BF16)
    scaled = contract(moved_rows(rows, per, own), scaled, 1, 0).astype(BF16)
    scaled_out[...] = scaled
    for k, given in enumerate((up, down)):
        copies[k].wait()
        for h, y in enumerate(blocked(coded(contract(scaled, theirs[k], 1, 0)), owners)):
            given[:, h * per : (h + 1) * per, :] = y


def keep_kernel(tokens, scaled_in, wq, wk, wv, wo, gates_hbm, keep_up, keep_down, small, gates, sem, *, owners):
    z, tp = lax.axis_index("kv"), lax.axis_index("tp")
    seqs, props, width = tokens.shape
    fetch = pltpu.make_async_copy(gates_hbm.at[:, :, pl.ds(pl.multiple_of(z * width, width), width)], gates, sem)
    fetch.start()
    rows = seqs * props
    per = rows // owners
    own = per // props
    x = tokens[...].astype(F32).reshape(rows, width)
    scaled = scaled_in[...]
    even = (z & 1) == 0
    for first, second, kept in ((wq, wk, keep_up), (wv, wo, keep_down)):
        ours = jnp.where(even, first[...], second[...])
        for h, y in enumerate(blocked(contract(scaled, ours, 1, 0), owners)):
            kept[:, h * per : (h + 1) * per, :] = y
    move = moved_rows(rows, per, own)
    square = x * x
    s_hi = square.astype(BF16)
    s_lo = (square - s_hi.astype(F32)).astype(BF16)
    ones = jnp.ones((8, width), BF16)
    s = contract(ones, contract(move, s_hi, 1, 0).astype(BF16), 1, 1)
    s += contract(ones, contract(move, s_lo, 1, 0).astype(BF16), 1, 1)
    fetch.wait()
    heads = gates.shape[1]
    local = heads // lax.axis_size("tp")
    pick_r, pick_c = iota((8, 2 * heads), 0), iota((8, 2 * heads), 1)
    want = ((pick_r & 3) // local) * heads + tp * local + (pick_r & (local - 1))
    pick = jnp.where(pick_c == want, 1.0, 0.0).astype(BF16)
    own_gates = contract(pick, gates[...].reshape(2 * heads, width), 1, 0).astype(BF16)
    g = contract(own_gates, scaled, 1, 1)

    def words(value, split):
        hi = value.astype(BF16).astype(F32)
        return jnp.where(iota(value.shape, 0) < split, hi, value - hi)

    g, s = words(g, 4), words(s, 1)
    lanes = iota((8, 128), 1)
    span = 128 // per
    for half in range(rows // 128):
        gh = g[:, half * 128 : (half + 1) * 128]
        sh = pltpu.roll(s[:, half * 128 : (half + 1) * 128], 64, 1)
        low = jnp.where(lanes < 64, gh, sh).astype(BF16)
        high = jnp.where(lanes < 64, sh, gh).astype(BF16)
        for k in range(span):
            small[half * span + k] = low if k < span // 2 else high


def merge_kernel(got_up, got_down, keep_up, keep_down, small, out, made, sems):
    owners, half, _ = got_up.shape
    quarter = owners // 4
    copies = []
    for part in range(4):
        own = slice(part * quarter, (part + 1) * quarter)
        for at, got, kept in ((0, got_up, keep_up), (half, got_down, keep_down)):
            made[own, at : at + half, :] = coded(kept[own] + decoded(got[own]) * (1.0 / SHIFT))
        made[own, 2 * half :, :] = small[own]
        copies.append(pltpu.make_async_copy(made.at[own], out.at[own], sems.at[part]))
        copies[part].start()
    for copy in copies:
        copy.wait()


def take_kernel(accepted, stab, ib, fb, memory_hbm, norms, m0, n0, words, move, bias, first, sems, *, owners, seqs):
    own, _, heads, dim, _ = m0.shape
    copies = []
    for b in range(own):
        copies.append(pltpu.make_async_copy(memory_hbm.at[b, accepted[b]], m0.at[b, 0], sems.at[b]))
        copies[b].start()
    col = iota(bias.shape[1:], 1)
    for k, source in enumerate((ib, fb)):
        value = jnp.zeros(bias.shape[1:], F32)
        for h in range(heads):
            value = jnp.where(col == h, source[h], value)
        bias[k] = value
    srow, scol = iota((own, heads), 0), iota((own, heads), 1)
    m = jnp.zeros((own, heads), F32)
    for b in range(own):
        for h in range(heads):
            m = jnp.where((srow == b) & (scol == h), stab[b, h, accepted[b]], m)
    first[...] = m
    rows = move.shape[0]
    props = rows // seqs
    per = rows // owners
    r, c = iota((rows, rows), 0), iota((rows, rows), 1)
    t, rest = c >> log2(seqs), c & (seqs - 1)
    place = (((rest >> log2(own)) - TURN[1][2]) * TURN[1][1]) & (owners - 1)
    source = place * per + t * own + (rest & (own - 1))
    move[...] = jnp.where(r == source, 1.0, 0.0).astype(BF16)
    for b in range(own):
        n0[b] = norms[b, accepted[b]]
        copies[b].wait()
        for h in range(heads):
            value = m0[b, 0, h]
            hi = value.astype(BF16)
            words[h, b * dim : (b + 1) * dim, :dim] = hi
            words[h, b * dim : (b + 1) * dim, dim:] = (value - hi.astype(F32)).astype(BF16)


def cell_kernel(got, words, n0, bias, start, gated, kv_out, coef, *, features):
    z = lax.axis_index("kv")
    owners = got.shape[0]
    own, heads, dim = n0.shape
    main = got.shape[1] - 8
    per = main // (2 * heads)
    props = per // own
    small = got[0, main:].astype(F32)
    for k in range(1, owners):
        small = small + got[k, main:].astype(F32)
    shift = (((z - TURN[0][2]) * TURN[0][1]) & (128 // per - 1)) * per
    small = pltpu.roll(small, (128 - shift) & 127, 1)
    g = small + pltpu.roll(small, 4, 0)
    sq = pltpu.roll(small + pltpu.roll(small, 7, 0), 64, 1)
    packed = jnp.where(iota(g.shape, 0) < 4, g, pltpu.roll(sq, 4, 0))
    cols = packed.T[:per]
    inverse = lax.rsqrt(cols[:, 4:5] / features + EPSILON)
    in_gate = cols[:, 0:2] * inverse + bias[0]
    f = cols[:, 2:4] * inverse + bias[1]
    log_forget = jnp.minimum(f, 0.0) - jnp.log1p(jnp.exp(-jnp.abs(f)))
    m = start[...]
    stabs, retain, admit = [m], [], []
    for t in range(props):
        carried = log_forget[t * own : (t + 1) * own] + m
        incoming = in_gate[t * own : (t + 1) * own]
        top = jnp.maximum(carried, incoming)
        retain.append(jnp.exp(carried - top))
        admit.append(jnp.exp(incoming - top))
        m = top
        stabs.append(m)
    scale = dim ** (-0.5)
    factor = inverse * (1.0 / SHIFT)
    rr = iota((per, dim), 0) & (own - 1)

    def part(kind, h):
        at = ((kind >> 1) * heads + h) * per
        first = (kind + TURN[0][2]) & 1
        total = decoded(got[first, at : at + per])
        for k in range(2 + first, owners, 2):
            total = total + decoded(got[k, at : at + per])
        return (total * factor).astype(BF16)

    outs = []
    for h in range(heads):
        q, k, v, o = part(0, h), part(1, h), part(2, h), part(3, h)
        kv_out[h] = k
        kv_out[heads + h] = v
        qf, kf, vf = q.astype(F32), k.astype(F32) * scale, v.astype(F32)
        wide = jnp.concatenate([jnp.where(rr == b, qf, 0.0) for b in range(own)], 1).astype(BF16)
        both = contract(wide, words[h], 1, 0)
        base = both[:, :dim] + both[:, dim:]
        norm = n0[:, h, :]
        rows = []
        for t in range(props):
            sl = slice(t * own, (t + 1) * own)
            norm = retain[t][:, h : h + 1] * norm + admit[t][:, h : h + 1] * kf[sl]
            den = jnp.sum(qf[sl] * norm, -1, keepdims=True)
            weight = jnp.ones((own, 1), F32)
            num = jnp.zeros((own, dim), F32)
            for s in range(t, -1, -1):
                ss = slice(s * own, (s + 1) * own)
                dots = jnp.sum(qf[sl] * kf[ss], -1, keepdims=True)
                num += (weight * admit[s][:, h : h + 1] * dots) * vf[ss]
                weight = weight * retain[s][:, h : h + 1]
            num += weight * base[sl]
            floor = jnp.exp(-stabs[t + 1][:, h : h + 1])
            rows.append(num / jnp.maximum(jnp.abs(den), floor))
        hidden = jnp.concatenate(rows, 0)
        outs.append(jax.nn.sigmoid(o.astype(F32)) * hidden)
    result = jnp.concatenate(outs, 1).astype(BF16)
    for k in range(gated.shape[0]):
        gated[k] = result
    for t in range(props + 1):
        last = t - 1 if t else 0
        coef[t] = jnp.concatenate([stabs[t], retain[last], admit[last]], 1)


def memory_kernel(coef, m0, n0, kv, new_m, new_n, new_s, made, sems):
    own, _, heads, dim, _ = m0.shape
    per = kv.shape[1]
    props = per // own
    steps = props + 1
    scale = dim ** (-0.5)
    row, col = iota((heads, steps), 0), iota((heads, steps), 1)
    row_at = iota((per, dim), 0)
    sent = []

    def send(source, b, t):
        copy = pltpu.make_async_copy(source, new_m.at[b, t], sems.at[b, t])
        copy.start()
        sent.append(copy)

    for b in range(own):
        send(m0.at[b, 0], b, 0)
    for b in range(own):
        stabs = jnp.zeros((heads, steps), F32)
        norms = []
        for h in range(heads):
            norms.append(n0[b, h : h + 1])
            new_n[b, 0, h : h + 1] = norms[h]
            for t in range(steps):
                stabs = jnp.where((row == h) & (col == t), coef[t, b, h], stabs)
        new_s[b] = stabs
        memories = [m0[b, 0, h] for h in range(heads)]
        for t in range(props):
            for h in range(heads):
                keep, add = coef[t + 1, b, heads + h], coef[t + 1, b, 2 * heads + h] * scale
                one = jnp.where(row_at == t * own + b, kv[h].astype(F32), 0.0)
                memories[h] = keep * memories[h] + add * contract(one.astype(BF16), kv[heads + h], 0, 0)
                norms[h] = keep * norms[h] + add * jnp.sum(one, 0, keepdims=True)
                made[b, t, h] = memories[h]
                new_n[b, t + 1, h : h + 1] = norms[h]
            send(made.at[b, t], b, t + 1)
    for copy in sent:
        copy.wait()


def mix_kernel(gathered, w, after, out):
    owners, per, _ = gathered.shape
    rows = owners * per
    y = contract(w[...], gathered[...].reshape(rows, gathered.shape[2]), 0, 1).astype(BF16)
    out[...] = y.reshape(out.shape)


def finish_kernel(got, move, out):
    total = got[0].astype(F32)
    for k in range(1, got.shape[0]):
        total = total + got[k].astype(F32)
    props, _, seqs = out.shape
    y = contract(total.astype(BF16), move[...], 1, 0).astype(BF16)
    for t in range(props):
        out[t] = y[:, t * seqs : (t + 1) * seqs]


def log2(n):
    assert n & (n - 1) == 0
    return n.bit_length() - 1


SMEM = pl.BlockSpec(memory_space=pltpu.SMEM)
VMEM = pl.BlockSpec(memory_space=pltpu.VMEM)


def held(shape, dtype):
    return pltpu.VMEM(shape, dtype)


def near(x):
    return pltpu.with_memory_space_constraint(x, pltpu.VMEM)


def local(
    tokens,
    norm_gain,
    w_query,
    w_key,
    w_value,
    w_outgate,
    gate_weight,
    input_bias,
    forget_bias,
    w_out,
    saved_memory,
    saved_normalizer,
    saved_stabilizer,
    accepted,
):
    owners, peers = lax.axis_size("kv"), lax.axis_size("tp")
    seqs, props, width = tokens.shape
    heads = input_bias.shape[0]
    own, saved, _, dim, _ = saved_memory.shape
    columns = w_query.shape[1]
    per = own * props
    gates = gate_weight.transpose(0, 2, 1)
    all_heads = gates.shape[1]

    def whole(shape):
        return pl.BlockSpec(shape, lambda *_: (0,) * len(shape))

    half = columns // 128 * per
    weights = (w_query, w_key, w_value, w_outgate)
    up, down, scaled = pl.pallas_call(
        functools.partial(give_kernel, owners=owners),
        in_specs=[VMEM] * 2 + [pl.BlockSpec(memory_space=pl.ANY)] * 4,
        out_specs=[VMEM] * 3,
        out_shape=[
            held((owners, half, 128), BF16),
            held((owners, half, 128), BF16),
            held((seqs * props, width), BF16),
        ],
        scratch_shapes=[pltpu.VMEM((2, *w_query.shape), BF16), pltpu.SemaphoreType.DMA((2,))],
        name="give",
    )(tokens, norm_gain.reshape(-1, 128), *weights)

    with_next = [(i, i ^ 1) for i in range(owners)]
    with_last = [(i, (((i + 1) ^ 1) - 1) % owners) for i in range(owners)]
    got_up = lax.ppermute(up, "kv", with_next)
    got_down = lax.ppermute(down, "kv", with_last)
    keep_up, keep_down, small = pl.pallas_call(
        functools.partial(keep_kernel, owners=owners),
        in_specs=[VMEM] * 6 + [pl.BlockSpec(memory_space=pl.ANY)],
        out_specs=[VMEM] * 3,
        out_shape=[
            held((owners, half, 128), F32),
            held((owners, half, 128), F32),
            held((owners, 8, 128), BF16),
        ],
        scratch_shapes=[pltpu.VMEM((2, all_heads, width), BF16), pltpu.SemaphoreType.DMA],
        cost_estimate=pl.CostEstimate(flops=80_000_000, bytes_accessed=1_000_000, transcendentals=0),
        name="keep",
    )(tokens, near(scaled), *weights, gates)
    send = pl.pallas_call(
        merge_kernel,
        in_specs=[VMEM] * 5,
        out_specs=[pl.BlockSpec(memory_space=pl.ANY)],
        out_shape=[jax.ShapeDtypeStruct((owners, 2 * half + 8, 128), BF16)],
        scratch_shapes=[pltpu.VMEM((owners, 2 * half + 8, 128), BF16), pltpu.SemaphoreType.DMA((4,))],
        name="merge",
    )(near(got_up), near(got_down), near(keep_up), near(keep_down), near(small))[0]

    turned = [[[(stride * k + start) % owners for k in range(owners)]] for stride, _, start in TURN]
    turned = [None if x[0] == list(range(owners)) else x for x in turned]
    got = lax.all_to_all(send, "kv", 0, 0, axis_index_groups=turned[0], tiled=True)

    stab = saved_stabilizer.transpose(0, 2, 1)
    m0, n0, words, move, bias, first = pl.pallas_call(
        functools.partial(take_kernel, owners=owners, seqs=seqs),
        in_specs=[SMEM] * 4 + [pl.BlockSpec(memory_space=pl.ANY), VMEM],
        out_specs=[VMEM] * 6,
        out_shape=[
            held((own, 1, heads, dim, dim), F32),
            held((own, heads, dim), F32),
            held((heads, own * dim, 2 * dim), BF16),
            held((seqs * props, seqs * props), BF16),
            held((2, per, heads), F32),
            held((own, heads), F32),
        ],
        scratch_shapes=[pltpu.SemaphoreType.DMA((own,))],
        cost_estimate=pl.CostEstimate(flops=40_000_000, bytes_accessed=1_000_000, transcendentals=0),
        name="take",
    )(accepted, stab, input_bias, forget_bias, saved_memory, saved_normalizer)
    steps = props + 1
    gated, kv, coef = pl.pallas_call(
        functools.partial(cell_kernel, features=float(owners * width)),
        in_specs=[VMEM] * 5,
        out_specs=[VMEM] * 3,
        out_shape=[
            held((owners, per, columns), BF16),
            held((2 * heads, per, dim), BF16),
            jax.ShapeDtypeStruct((steps, own, 3 * heads), F32),
        ],
        name="cell",
    )(near(got), near(words), near(n0), near(bias), near(first))

    gathered = lax.all_to_all(gated, "kv", 0, 0, axis_index_groups=turned[1], tiled=True)

    new_memory, new_n, new_s = pl.pallas_call(
        memory_kernel,
        in_specs=[SMEM] + [VMEM] * 3,
        out_specs=[pl.BlockSpec(memory_space=pl.ANY), VMEM, VMEM],
        out_shape=[
            jax.ShapeDtypeStruct((own, steps, heads, dim, dim), F32),
            jax.ShapeDtypeStruct((own, steps, heads, dim), F32),
            jax.ShapeDtypeStruct((own, heads, steps), F32),
        ],
        scratch_shapes=[pltpu.VMEM((own, props, heads, dim, dim), F32), pltpu.SemaphoreType.DMA((own, steps))],
        cost_estimate=pl.CostEstimate(flops=20_000_000, bytes_accessed=3_200_000, transcendentals=0),
        name="memory",
    )(coef, near(m0), near(n0), near(kv))

    terms = pl.pallas_call(
        mix_kernel,
        in_specs=[VMEM] * 2 + [pl.BlockSpec(memory_space=pl.ANY)],
        out_specs=[VMEM],
        out_shape=[held((peers, w_out.shape[1] // peers, seqs * props), BF16)],
        name="mix",
    )(near(gathered), near(w_out), new_s)[0]
    arrived = lax.all_to_all(terms, "tp", split_axis=0, concat_axis=0, tiled=True)

    mixed = pl.pallas_call(
        finish_kernel,
        in_specs=[VMEM] * 2,
        out_specs=VMEM,
        out_shape=jax.ShapeDtypeStruct((props, w_out.shape[1] // peers, seqs), BF16),
        name="finish",
    )(near(arrived), near(move))
    return mixed.transpose(2, 0, 1), new_memory, new_n, new_s.transpose(0, 2, 1)


def solution(mesh):
    return jax.shard_map(
        local,
        mesh=mesh,
        in_specs=(
            P("grp", None, "kv"),
            P(),
            P("kv", "tp"),
            P("kv", "tp"),
            P("kv", "tp"),
            P("kv", "tp"),
            P(),
            P("tp"),
            P("tp"),
            P("tp", "kv"),
            P(("grp", "kv"), None, "tp", None, None),
            P(("grp", "kv"), None, "tp", None),
            P(("grp", "kv"), None, "tp"),
            P(("grp", "kv")),
        ),
        out_specs=(
            P("grp", None, ("kv", "tp")),
            P(("grp", "kv"), None, "tp", None, None),
            P(("grp", "kv"), None, "tp", None),
            P(("grp", "kv"), None, "tp"),
        ),
        check_vma=False,
    )
```
